256 devices in a mesh: ep: 64 (over z, x, core), tp: 4 (over y).
Axes of the slice: x: 4, y: 4, z: 8, core: 2. Of those that a mesh axis runs over, the one named last changes fastest.
Arguments:
- tokens: bfloat16 [32768, 4096], P('ep', 'tp'), may hold values from -100 to 100, as said below
- routes: int32 [32768, 2], P('ep'), may hold values from 0 to 127, all different within a row; in each aligned block of 512 rows (0 to 511, 512 to 1023, ...) at most 16 rows name the same one
- route_weights: float32 [32768, 2], P('ep'), may hold values from 0.1 to 1
- norm_gain: float32 [4096], P('tp'), may hold values from 0.1 to 1.9
- gate_weight: bfloat16 [128, 4096, 512], P('ep', 'tp'), may hold values from -0.09375 to 0.09375
- up_weight: bfloat16 [128, 4096, 512], P('ep', 'tp'), may hold values from -0.09375 to 0.09375
- down_weight: bfloat16 [128, 512, 4096], P('ep', None, 'tp'), may hold values from -0.25 to 0.25
- final_gain: float32 [4096], P('tp'), may hold values from 0.1 to 1.9
Outputs:
- mixed: bfloat16 [32768, 4096], P('ep', 'tp')
The draws below stay inside these ranges and needn't reach their ends.
Inputs may be any that keep to these rules, and one draw needn't show every extreme that they name: `tokens`: real-valued activations whose features differ in scale. `routes`: each row names 2 different experts; among the 512 rows of one aligned block no expert is named more than 16 times, a bound that some block reaches.
All inputs are finite; a program needn't handle non-finite values.
Results may differ from the reference program's by a relative error of at most 0.018.
Values may be sent and summed in bfloat16 or wider, within the bound.
A program may use at most 64 MiB of HBM per device.

```python
import math
import jax
import jax.numpy as jnp
import numpy as np
from jax import lax

D = 4096
FF = 512
TOP = 2
TOK_DEV = 512
EXPERTS = 128
CAP = 16
TOKENS = 32768
N_EP = 64
N_TP = 4


def draw_tokens(key, part):
    keys = jax.random.split(jax.random.fold_in(key, 11), 2)
    column = jnp.exp(jnp.log(6.0) * jnp.arange(D, dtype=jnp.float32) / (D - 1))
    row_scale = jnp.exp(jax.random.uniform(keys[1], (TOKENS, 1), jnp.float32, 0.0, jnp.log(10.0)))
    base = jax.random.normal(keys[0], (TOKENS, D), jnp.float32)
    base = jnp.clip(base, -5.0, 5.0)
    return (base * column * row_scale / 3.0).astype(jnp.bfloat16)


def shard_levels(own_key, dims, shards, smallest, high):
    loudness = 1.0
    for dim, blocks in shards:
        draws = jax.random.uniform(jax.random.fold_in(jax.random.fold_in(own_key, 6), dim), (blocks,), jnp.float32, smallest / len(shards), high / len(shards))
        loudness = loudness * jnp.repeat(jnp.exp(draws), dims[dim] // blocks).reshape((-1,) + (1,) * (len(dims) - 1 - dim))
    return loudness


def assign_block(key, own, number, rows, amount, top, limit, skew):
    order = jax.random.permutation(key, amount)
    crowded, ordinary = shares(amount, rows * top, limit, skew, True), shares(amount, rows * top, limit, skew, False)
    places = jnp.arange(amount)

    def named(tallies, offset_by):
        used = int((tallies > 0).sum())
        fixed = max(1, used // 4)
        shifted = fixed + (places - fixed + offset_by * (used - fixed)) % max(1, amount - fixed)
        return jnp.zeros((amount,), jnp.int32).at[order[jnp.where(places < fixed, places, shifted)]].set(jnp.asarray(tallies, jnp.int32))

    tallies = jnp.where(number % 4 == 0, named(crowded, number // 4), named(ordinary, number - number // 4 - 1))
    mixed = jax.random.permutation(jax.random.fold_in(own, 3), amount)
    source_of, sink = mixed[0:amount // 2 * 2:2], mixed[1:amount // 2 * 2:2]
    room = jnp.minimum(tallies[source_of] - 1, limit - tallies[sink]) // 2
    room = jnp.where((source_of == order[0]) | (sink == order[0]) | (tallies[sink] == 0), 0, jnp.maximum(room, 0))
    shifted = jax.random.randint(jax.random.fold_in(own, 4), (amount // 2,), 0, 1 << 20) % (room + 1)
    tallies = tallies.at[source_of].add(-shifted).at[sink].add(shifted)
    labels = jnp.searchsorted(jnp.cumsum(tallies), jnp.arange(rows * top), side="right").astype(jnp.int32)
    listing = labels.reshape(top, rows).T
    listing = listing[jax.random.permutation(jax.random.fold_in(own, 1), rows)]
    offset_by = jax.random.randint(jax.random.fold_in(own, 2), (rows, 1), 0, top)
    return jnp.take_along_axis(listing, (jnp.arange(top)[None, :] + offset_by) % top, axis=1)


def shares(amount, total, reach, lean, full):
    loads = [(1 << 20) // math.isqrt(grade ** lean) + 1 for grade in range(1, amount + 1)]
    largest = reach if full else min(reach, max(-(-total // amount), total * loads[0] // sum(loads)))
    least = 1 if total - largest >= amount - 1 else 0
    given, surplus = [largest] + [least] * (amount - 1), total - largest - least * (amount - 1)
    while surplus > 0:
        candidates = [i for i in range(1, amount) if given[i] < largest] or [i for i in range(1, amount) if given[i] < reach]
        pool, left = sum([loads[i] for i in candidates]), surplus
        for i in candidates:
            addition = min(reach - given[i], max(1, left * loads[i] // pool), surplus)
            given[i] = given[i] + addition
            surplus = surplus - addition
    return np.array(given)


def noise(key, shape, scale, bound, pieces=(), kind=jnp.bfloat16):
    result = scale * jax.random.normal(key, shape, jnp.float32)
    if pieces:
        result = result * shard_levels(key, shape, pieces, -0.22, 0.18)
    return jnp.clip(result, -bound, bound).astype(kind)


def setup_inputs(seed: int = 0) -> dict:
    arg_keys = jax.random.split(jax.random.key(seed), 9)
    tokens = draw_tokens(jax.random.fold_in(arg_keys[8], 71), 0)
    routes_keys = jax.random.split(jax.random.fold_in(arg_keys[1], 1), TOKENS // TOK_DEV)
    routes_turns = jax.random.permutation(jax.random.fold_in(arg_keys[1], 3), TOKENS // TOK_DEV)
    routes = jax.vmap(lambda own, number: assign_block(jax.random.fold_in(arg_keys[1], 2), own, number, TOK_DEV, EXPERTS, TOP, CAP, 2))(routes_keys, routes_turns).reshape((TOKENS, TOP))
    route_weights = jnp.clip(0.1 + 0.9 * jax.random.uniform(arg_keys[2], (TOKENS, TOP), jnp.float32) ** shard_levels(arg_keys[2], (TOKENS, TOP), ((0, 64),), -0.2, 0.2), 0.1, 1.0)
    norm_gain = jnp.clip(1.0 + 0.18 * jax.random.normal(arg_keys[3], (D,), jnp.float32), 0.1, 1.9)
    gate_weight = noise(arg_keys[4], (EXPERTS, D, FF), D ** -0.5, 0.09375, ((0, 64), (1, 4)))
    up_weight = noise(arg_keys[5], (EXPERTS, D, FF), D ** -0.5, 0.09375, ((0, 64), (1, 4)))
    down_weight = noise(arg_keys[6], (EXPERTS, FF, D), FF ** -0.5, 0.25, ((0, 64), (2, 4)))
    final_gain = jnp.clip(1.0 + 0.18 * jax.random.normal(arg_keys[7], (D,), jnp.float32), 0.1, 1.9)
    return {"tokens": tokens, "routes": routes, "route_weights": route_weights, "norm_gain": norm_gain, "gate_weight": gate_weight, "up_weight": up_weight, "down_weight": down_weight, "final_gain": final_gain}


EPSILON = 1e-06

def slots_of(chosen):
    experts = jnp.arange(EXPERTS, dtype=jnp.int32)
    onehot = (chosen[:, None] == experts[None, :]).astype(jnp.int32)
    before = jnp.cumsum(onehot, axis=0) - onehot
    return lax.optimization_barrier(jnp.sum(before * onehot, axis=1)).astype(jnp.int32)

def reference(tokens, routes, route_weights, norm_gain, gate_weight, up_weight, down_weight, final_gain):
    values = tokens.astype(jnp.float32)
    scale = lax.rsqrt(lax.optimization_barrier(jnp.mean(values * values, axis=-1, keepdims=True)) + EPSILON)
    normed = (values * scale * norm_gain).astype(jnp.bfloat16)
    count = tokens.shape[0]
    blocks = routes.reshape(N_EP, TOK_DEV * TOP)
    slots = jax.vmap(slots_of)(blocks)
    source = jnp.broadcast_to(jnp.arange(N_EP, dtype=jnp.int32)[:, None], blocks.shape)
    owner = source * TOK_DEV + jnp.arange(TOK_DEV * TOP, dtype=jnp.int32)[None, :] // TOP
    table = jnp.full((EXPERTS, N_EP, CAP), count, jnp.int32).at[blocks, source, slots].set(owner)
    padded = jnp.concatenate([normed, jnp.zeros((1, D), jnp.bfloat16)], axis=0)
    block_width = D // N_TP

    def one_expert(operands):
        index, w_gate, w_up, w_down = operands
        rows = padded[index.reshape(-1)]
        gate = jnp.zeros((rows.shape[0], FF), jnp.float32)
        upper = jnp.zeros((rows.shape[0], FF), jnp.float32)
        for quarter in range(N_TP):
            lower_col = quarter * block_width
            part_rows = rows[:, lower_col:lower_col + block_width]
            gate = gate + jnp.dot(part_rows, w_gate[lower_col:lower_col + block_width], preferred_element_type=jnp.float32).astype(jnp.bfloat16).astype(jnp.float32)
            upper = upper + jnp.dot(part_rows, w_up[lower_col:lower_col + block_width], preferred_element_type=jnp.float32).astype(jnp.bfloat16).astype(jnp.float32)
        hidden = (jax.nn.silu(gate) * upper).astype(jnp.bfloat16)
        return jnp.dot(hidden, w_down, preferred_element_type=jnp.float32).astype(jnp.bfloat16)
    outputs = lax.map(one_expert, (table, gate_weight, up_weight, down_weight))
    returned = outputs.reshape(EXPERTS * N_EP * CAP, D)
    position = (blocks * (N_EP * CAP) + source * CAP + slots).reshape(count, TOP)
    combined = jnp.zeros((count, D), jnp.float32)
    for which in range(TOP):
        combined = combined + route_weights[:, which:which + 1] * returned[position[:, which]].astype(jnp.float32)
    closing = lax.rsqrt(lax.optimization_barrier(jnp.mean(combined * combined, axis=-1, keepdims=True)) + EPSILON)
    return (combined * closing * final_gain).astype(jnp.bfloat16)
```

```python
import functools

import jax
import jax.numpy as jnp
from jax import lax
from jax.experimental import pallas as pl
from jax.experimental.pallas import tpu as pltpu
from jax.sharding import PartitionSpec as P

EPSILON = 1e-06
NZ = 8
F32 = jnp.float32
BF16 = jnp.bfloat16
I32 = jnp.int32


def layer_kernel(
    NP, NT, tok, rts, rws, ngain, fgain, gw, uw, dw, out,
    X0, DB, TG, TR, XS, XR, PS, PR, GS, GR, HB, OS, OR, FN, RL, ACC, WGU, WD, SQ, SQ2,
    w_sem, sq_s, sq_r, tg_s, tg_r, db_s, db_r, ps_s, ps_r, x_s, x_r, g_s, g_r, h_s, h_r,
    o_s, o_r, f_s, f_r, rl_s, rl_r,
):
    T, W = tok.shape
    HALF = T // 2
    CAP = TR_CAP(T, NP)
    G2 = 2 * CAP
    RP = NP * G2
    M = NP * CAP
    FQ = WGU.shape[3] // 2
    CB = 256 if W % 256 == 0 else 128
    NB = W // CB
    D = W * NT
    ep = lax.axis_index("ep")
    y = lax.axis_index("tp")
    z = ep // NP
    p = ep % NP

    def zz(o):
        return (z + (o + NZ)) % NZ

    def zdev(o):
        return {"ep": zz(o) * NP + p}

    def pdev(j):
        return {"ep": z * NP + (p + j) % NP}

    def tdev(j):
        return {"tp": (y + j) % NT}

    def send(src, dst, ss, rs, dev):
        pltpu.make_async_remote_copy(
            src_ref=src, dst_ref=dst, send_sem=ss, recv_sem=rs,
            device_id=dev, device_id_type=pl.DeviceIdType.MESH,
        ).start()

    def wait(ref, sem):
        pltpu.make_async_copy(ref, ref, sem).wait()

    barrier = pltpu.get_barrier_semaphore()
    partners = [zdev(o) for o in range(1, NZ)] + [pdev(j) for j in range(1, NP)]
    partners += [tdev(j) for j in range(1, NT)]
    for dev in partners:
        pl.semaphore_signal(barrier, inc=1, device_id=dev, device_id_type=pl.DeviceIdType.MESH)

    for m in range(2):
        for q in range(NT):
            cols = pl.ds(q * FQ, FQ)
            pltpu.make_async_copy(gw.at[m, :, cols], WGU.at[m, q, :, pl.ds(0, FQ)], w_sem.at[0]).start()
            pltpu.make_async_copy(uw.at[m, :, cols], WGU.at[m, q, :, pl.ds(FQ, FQ)], w_sem.at[0]).start()
    pltpu.make_async_copy(dw, WD, w_sem.at[1]).start()

    TB = min(128, T)

    def squares(load, buf):
        for b in range(T // TB):
            v = load(b)
            s = jnp.sum(v * v, axis=1, keepdims=True)
            row = jnp.transpose(jnp.broadcast_to(s, (TB, 128)))
            buf[y, :, b * TB:(b + 1) * TB] = row[0:8, :]

    def share(buf, k):
        for j in range(1, NT):
            send(buf.at[y], buf.at[y], sq_s.at[k], sq_r.at[k], tdev(j))

    def scales(buf, b):
        total = buf[0, :, b * TB:(b + 1) * TB]
        for q in range(1, NT):
            total = total + buf[q, :, b * TB:(b + 1) * TB]
        s = lax.rsqrt(total / D + EPSILON)
        return jnp.transpose(jnp.broadcast_to(s[0:1, :], (128, TB)))

    squares(lambda b: tok[b * TB:(b + 1) * TB, :].astype(F32), SQ)
    pl.semaphore_wait(barrier, len(partners))
    share(SQ, 0)

    r0 = rts[0:1, :]
    r1 = rts[1:2, :]
    NE = NZ * NP * 2
    eio = lax.broadcasted_iota(I32, (NE, T), 0)
    oh0 = jnp.where(eio == r0, 1.0, 0.0)
    oh1 = jnp.where(eio == r1, 1.0, 0.0)
    up = jnp.where(
        lax.broadcasted_iota(I32, (T, T), 0) < lax.broadcasted_iota(I32, (T, T), 1), 1.0, 0.0
    ).astype(BF16)
    before = jnp.dot((oh0 + oh1).astype(BF16), up, preferred_element_type=F32)
    t0 = r0 * CAP + jnp.sum(oh0 * before, axis=0, keepdims=True).astype(I32)
    t1 = r1 * CAP + jnp.sum(oh1 * before, axis=0, keepdims=True).astype(I32)
    TG[...] = jnp.where(lax.broadcasted_iota(I32, (8, T), 0) == 0, t0, t1)
    for slot, o in enumerate((1, -1, 2, -2)):
        send(TG, TR.at[slot], tg_s, tg_r.at[slot], zdev(o))

    wait(SQ.at[pl.ds(0, NT - 1)], sq_r.at[0])
    for h in range(2):
        for b in range(h * HALF // TB, (h + 1) * HALF // TB):
            sc = scales(SQ, b)
            for c in range(W // 128):
                cc = slice(c * 128, (c + 1) * 128)
                v = tok[b * TB:(b + 1) * TB, cc].astype(F32) * sc * ngain[0:1, cc]
                X0[h, b * TB - h * HALF:(b + 1) * TB - h * HALF, cc] = v.astype(BF16)
        send(X0.at[h], DB.at[0, h], db_s.at[0, h], db_r.at[0, h], zdev(1))
        send(X0.at[h], DB.at[1, h], db_s.at[1, h], db_r.at[1, h], zdev(-1))

    def pick(targets, rows, base, xref, dst):
        a = targets[0:1, :]
        b = targets[1:2, :]
        at = lax.broadcasted_iota(I32, (rows, T), 0) + base
        sel = jnp.where((at == a) | (at == b), 1.0, 0.0).astype(BF16)

        def cols(n, carry):
            cc = pl.ds(pl.multiple_of(n * CB, CB), CB)
            got = jnp.dot(sel[:, :HALF], xref[0, :, cc], preferred_element_type=F32)
            got = got + jnp.dot(sel[:, HALF:], xref[1, :, cc], preferred_element_type=F32)
            dst[:, :, cc] = got.astype(BF16).reshape(rows // G2, G2, CB)
            return carry

        lax.fori_loop(0, NB, cols, 0)

    def to_plane(i, src):
        for j in range(1, NP):
            send(src.at[(p + j) % NP], XR.at[i, p], x_s.at[i], x_r.at[i], pdev(j))
        XR[i, p] = src[p]

    def stage_a(i):
        if i == 0:
            pick(TG[...], RP, z * RP, X0, XS.at[0])
        elif i <= 4:
            pick(TR[i - 1], RP, z * RP, DB.at[i - 1], XS.at[i])
        else:
            if i < 7:
                wait(PR.at[i - 5], ps_r.at[i - 5])
            else:
                wait(PR.at[2, pl.ds(0, NP // 2)], ps_r.at[2])
                wait(PR.at[2, pl.ds(NP // 2, NP // 2)], ps_r.at[3])
        to_plane(i, XS.at[i] if i <= 4 else PR.at[i - 5])

    def forward(h):
        wait(DB.at[0, h], db_r.at[0, h])
        send(DB.at[0, h], DB.at[2, h], db_s.at[2, h], db_r.at[2, h], zdev(1))
        wait(DB.at[1, h], db_r.at[1, h])
        send(DB.at[1, h], DB.at[3, h], db_s.at[3, h], db_r.at[3, h], zdev(-1))

    def far(k):
        step = 1 - 2 * k
        for h in range(2):
            wait(DB.at[2 + k, h], db_r.at[2 + k, h])
        wait(TR.at[2 + k], tg_r.at[2 + k])
        pick(TR[2 + k], RP, zz(step) * RP, DB.at[2 + k], PS.at[k, pl.ds(0, NP)])
        send(PS.at[k, pl.ds(0, NP)], PR.at[k], ps_s.at[k, 0], ps_r.at[k], zdev(step))
        H = NP // 2
        pick(TR[2 + k], RP // 2, zz(2 * step) * RP + k * (RP // 2), DB.at[2 + k], PS.at[k, pl.ds(NP, H)])
        send(PS.at[k, pl.ds(NP, H)], PR.at[2, pl.ds(k * H, H)], ps_s.at[k, 1], ps_r.at[2 + k], zdev(2 * step))

    def stage_b(i):
        wait(XR.at[i, pl.ds(0, NP - 1)], x_r.at[i])

        def one(j, carry):
            q = (y + 1 + j) % NT
            for m in range(2):
                rows = XR[i, :, m * CAP:(m + 1) * CAP, :].reshape(M, W)
                got = jnp.dot(rows, WGU[m, q], preferred_element_type=F32)
                GS[i, q, m] = got.astype(BF16)

            @pl.when(j < NT - 1)
            def _():
                send(GS.at[i, q], GR.at[i, y], g_s.at[i], g_r.at[i], {"tp": q})

            return carry

        lax.fori_loop(0, NT, one, 0)

    def stage_c(i):
        wait(GR.at[i, pl.ds(0, NT - 1)], g_r.at[i])
        for m in range(2):
            total = GS[i, y, m].astype(F32)
            for j in range(1, NT):
                total = total + GR[i, (y + j) % NT, m].astype(F32)
            gate = total[:, :FQ]
            HB[i, y, m] = (gate / (1.0 + jnp.exp(-gate)) * total[:, FQ:]).astype(BF16)
        for j in range(1, NT):
            send(HB.at[i, y], HB.at[i, y], h_s.at[i], h_r.at[i], tdev(j))

    def stage_d(i):
        wait(HB.at[i, pl.ds(0, NT - 1)], h_r.at[i])
        for m in range(2):
            hid = jnp.concatenate([HB[i, q, m] for q in range(NT)], axis=1)

            def cols(n, carry):
                cc = pl.ds(pl.multiple_of(n * CB, CB), CB)
                got = jnp.dot(hid, WD[m, :, cc], preferred_element_type=F32)
                OS[i, :, m * CAP:(m + 1) * CAP, cc] = got.astype(BF16).reshape(NP, CAP, CB)
                return carry

            lax.fori_loop(0, NB, cols, 0)
        for j in range(1, NP):
            d = (p + j) % NP
            send(OS.at[i, d], OR.at[i, p], o_s.at[i], o_r.at[i], pdev(j))
        OR[i, p] = OS[i, p]

    offs = (0, -1, 1, -2, 2, -3, 3, 4)

    def stage_e(i):
        wait(OR.at[i, pl.ds(0, NP - 1)], o_r.at[i])
        if 0 < i < 7:
            send(OR.at[i], FN.at[z], f_s.at[i, 0], f_r.at[i, 0], zdev(offs[i]))
        if i == 7:
            H = NP // 2
            for k in range(2):
                send(OR.at[7, pl.ds(k * H, H)], RL.at[k], f_s.at[7, k], rl_r.at[k], zdev(1 - 2 * k))

    def relay(k):
        H = NP // 2
        s = 1 - 2 * k
        wait(RL.at[k], rl_r.at[k])
        send(RL.at[k], FN.at[zz(-s), pl.ds(k * H, H)], rl_s.at[k], f_r.at[7, k], zdev(3 * s))

    def combine(i):
        if i == 0:
            src, plane = OR.at[0], z
        else:
            plane = zz(-offs[i])
            src = FN.at[plane]
            if i < 7:
                wait(src, f_r.at[i, 0])
            else:
                for k in range(2):
                    wait(src.at[pl.ds(k * (NP // 2), NP // 2)], f_r.at[7, k])
        for b in range(T // TB):
            bb = slice(b * TB, (b + 1) * TB)
            cols = []
            for row in (TG[0:1, bb].astype(F32), TG[1:2, bb].astype(F32), rws[0:1, bb], rws[1:2, bb]):
                cols.append(jnp.transpose(jnp.broadcast_to(row, (128, TB))))
            mat = []
            for c in range(RP // 128):
                at = (lax.broadcasted_iota(I32, (TB, 128), 1) + (plane * RP + c * 128)).astype(F32)
                mat.append(jnp.where(at == cols[0], cols[2], 0.0) + jnp.where(at == cols[1], cols[3], 0.0))
            mat = jnp.concatenate(mat, axis=1).astype(BF16)

            def accumulate(n, carry):
                cc = pl.ds(pl.multiple_of(n * CB, CB), CB)
                got = jnp.dot(mat, src[:, :, cc].reshape(RP, CB), preferred_element_type=F32)
                if i == 0:
                    ACC[bb, cc] = got
                else:
                    ACC[bb, cc] = ACC[bb, cc] + got
                return carry

            lax.fori_loop(0, NB, accumulate, 0)

    stage_a(0)
    wait(WGU, w_sem.at[0])
    wait(WD, w_sem.at[1])
    stage_b(0)
    forward(0)
    stage_c(0)
    stage_d(0)
    forward(1)
    wait(TR.at[0], tg_r.at[0])
    stage_a(1)
    wait(TR.at[1], tg_r.at[1])
    stage_a(2)
    stage_e(0)
    stage_b(1)
    stage_b(2)
    stage_c(1)
    stage_c(2)
    stage_d(1)
    far(0)
    far(1)
    stage_a(3)
    stage_a(4)
    stage_d(2)
    stage_e(1)
    stage_b(3)
    stage_e(2)
    stage_b(4)
    stage_c(3)
    stage_c(4)
    stage_a(5)
    stage_a(6)
    stage_d(3)
    stage_d(4)
    stage_a(7)
    stage_b(5)
    stage_b(6)
    stage_e(3)
    stage_e(4)
    stage_c(5)
    stage_c(6)
    stage_b(7)
    stage_d(5)
    stage_d(6)
    stage_c(7)
    stage_e(5)
    stage_e(6)
    stage_d(7)
    combine(0)
    stage_e(7)
    combine(1)
    combine(2)
    relay(0)
    relay(1)
    for i in range(3, NZ):
        combine(i)

    squares(lambda b: ACC[b * TB:(b + 1) * TB, :], SQ2)
    share(SQ2, 1)
    wait(SQ2.at[pl.ds(0, NT - 1)], sq_r.at[1])
    for b in range(T // TB):
        sc = scales(SQ2, b)
        for c in range(W // 128):
            cc = slice(c * 128, (c + 1) * 128)
            out[b * TB:(b + 1) * TB, cc] = (ACC[b * TB:(b + 1) * TB, cc] * sc * fgain[0:1, cc]).astype(BF16)

    for k in range(2):
        wait(SQ.at[pl.ds(0, NT - 1)], sq_s.at[k])
        wait(RL.at[k], rl_s.at[k])
        wait(RL.at[k], f_s.at[7, k])
        wait(PR.at[k], ps_s.at[k, 0])
        wait(RL.at[k], ps_s.at[k, 1])
    wait(TR, tg_s)
    for k in range(4):
        for h in range(2):
            wait(DB.at[k, h], db_s.at[k, h])
    for i in range(NZ):
        wait(XR.at[i, pl.ds(0, NP - 1)], x_s.at[i])
        wait(GR.at[i, pl.ds(0, NT - 1)], g_s.at[i])
        wait(HB.at[i, pl.ds(0, NT - 1)], h_s.at[i])
        wait(OR.at[i, pl.ds(0, NP - 1)], o_s.at[i])
        if 0 < i < 7:
            wait(OR.at[i], f_s.at[i, 0])


def TR_CAP(rows, planar):
    return 4 * rows // (NZ * planar * 2)


def body(tokens, routes, route_weights, norm_gain, gate_weight, up_weight, down_weight, final_gain):
    NT = lax.axis_size("tp")
    NP = lax.axis_size("ep") // NZ
    T, W = tokens.shape
    FF = gate_weight.shape[2]
    FQ = FF // NT
    CAP = TR_CAP(T, NP)
    G2 = 2 * CAP
    M = NP * CAP
    rows = (NP, G2, W)
    vm = pltpu.VMEM
    dma = pltpu.SemaphoreType.DMA
    scratch = [
        vm((2, T // 2, W), BF16),
        vm((4, 2, T // 2, W), BF16),
        vm((8, T), I32),
        vm((4, 8, T), I32),
        vm((5, *rows), BF16),
        vm((NZ, *rows), BF16),
        vm((2, NP + NP // 2, G2, W), BF16),
        vm((3, *rows), BF16),
        vm((NZ, NT, 2, M, 2 * FQ), BF16),
        vm((NZ, NT, 2, M, 2 * FQ), BF16),
        vm((NZ, NT, 2, M, FQ), BF16),
        vm((NZ, *rows), BF16),
        vm((NZ, *rows), BF16),
        vm((NZ, *rows), BF16),
        vm((2, NP // 2, G2, W), BF16),
        vm((T, W), F32),
        vm((2, NT, W, 2 * FQ), BF16),
        vm((2, FF, W), BF16),
        vm((NT, 8, T), F32),
        vm((NT, 8, T), F32),
        dma((2,)),
        dma((2,)), dma((2,)),
        dma, dma((4,)),
        dma((4, 2)), dma((4, 2)),
        dma((2, 2)), dma((4,)),
        dma((NZ,)), dma((NZ,)),
        dma((NZ,)), dma((NZ,)),
        dma((NZ,)), dma((NZ,)),
        dma((NZ,)), dma((NZ,)),
        dma((NZ, 2)), dma((NZ, 2)),
        dma((2,)), dma((2,)),
    ]
    v = pl.BlockSpec(memory_space=pltpu.VMEM)
    a = pl.BlockSpec(memory_space=pl.ANY)
    return pl.pallas_call(
        functools.partial(layer_kernel, NP, NT),
        out_shape=jax.ShapeDtypeStruct((T, W), BF16),
        in_specs=[v, v, v, v, v, a, a, a],
        out_specs=v,
        scratch_shapes=scratch,
        compiler_params=pltpu.CompilerParams(
            collective_id=0, has_side_effects=True, vmem_limit_bytes=67043328
        ),
    )(
        tokens, routes.T, route_weights.T, norm_gain[None], final_gain[None],
        gate_weight, up_weight, down_weight,
    )


def solution(mesh):
    in_specs = (
        P("ep", "tp"),
        P("ep", None),
        P("ep", None),
        P("tp"),
        P("ep", "tp", None),
        P("ep", "tp", None),
        P("ep", None, "tp"),
        P("tp"),
    )
    out_specs = P("ep", "tp")
    return jax.shard_map(body, mesh=mesh, in_specs=in_specs, out_specs=out_specs, check_vma=False)
```

```python
import functools

import jax
import jax.numpy as jnp
from jax import lax
from jax.experimental import pallas as pl
from jax.experimental.pallas import tpu as pltpu
from jax.sharding import PartitionSpec as P

EPSILON = 1e-06
NZ = 8
F32 = jnp.float32
BF16 = jnp.bfloat16
I32 = jnp.int32


def layer_kernel(
    NP, NT, tok, rts, rws, ngain, fgain, gw, uw, dw, out,
    DB, MT, MR, XS, XR, PS, GS, GR, HB, OS, OR, RV, CO, CM, RS, RD, ACC, WGU, WD, SQ, SQ2,
    w_sem, sq_s, sq_r, mt_s, mt_r, db_s, db_r, ps_s, x_s, x_r, g_s, g_r, h_s, h_r,
    o_s, o_r, rv_r, rd_s, rd_r,
):
    T, W = tok.shape
    HALF = T // 2
    CAP = cap_of(T, NP)
    G2 = 2 * CAP
    RP = NP * G2
    M = NP * CAP
    FQ = WGU.shape[3] // 2
    CB = RS.shape[3]
    NB = W // CB
    D = W * NT
    H = NP // 2
    NE = NZ * NP
    TB = min(128, T)
    ep = lax.axis_index("ep")
    y = lax.axis_index("tp")
    z = ep // NP
    p = ep % NP
    par = p % 2
    MESH = pl.DeviceIdType.MESH

    def zz(o):
        return (z + o + NZ) % NZ

    def at_plane(o, q):
        return {"ep": zz(o) * NP + q}

    def tdev(j):
        return {"tp": (y + j) % NT}

    def send(src, dst, ss, rs, dev):
        pltpu.make_async_remote_copy(
            src_ref=src, dst_ref=dst, send_sem=ss, recv_sem=rs, device_id=dev, device_id_type=MESH,
        ).start()

    def wait(ref, sem):
        pltpu.make_async_copy(ref, ref, sem).wait()

    barrier = pltpu.get_barrier_semaphore()

    def greet(j, carry):
        pl.semaphore_signal(barrier, inc=1, device_id={"ep": (ep + j) % NE}, device_id_type=MESH)
        return carry

    lax.fori_loop(1, NE, greet, 0)
    for j in range(1, NT):
        pl.semaphore_signal(barrier, inc=1, device_id=tdev(j), device_id_type=MESH)

    for m in range(2):
        for q in range(NT):
            cols = pl.ds(q * FQ, FQ)
            pltpu.make_async_copy(gw.at[m, :, cols], WGU.at[m, q, :, pl.ds(0, FQ)], w_sem.at[0]).start()
            pltpu.make_async_copy(uw.at[m, :, cols], WGU.at[m, q, :, pl.ds(FQ, FQ)], w_sem.at[0]).start()
    pltpu.make_async_copy(dw, WD, w_sem.at[1]).start()

    def squares(load, buf):
        for b in range(T // TB):
            v = load(b)
            s = jnp.sum(v * v, axis=1, keepdims=True)
            row = jnp.transpose(jnp.broadcast_to(s, (TB, 128)))
            buf[y, :, b * TB:(b + 1) * TB] = row[0:8, :]

    def share(buf, k):
        for j in range(1, NT):
            send(buf.at[y], buf.at[y], sq_s.at[k], sq_r.at[k], tdev(j))

    def scale_rows(buf):
        total = buf[0]
        for q in range(1, NT):
            total = total + buf[q]
        return lax.rsqrt(total / D + EPSILON)

    def send_h(h):
        part = tok.at[pl.ds(h * HALF, HALF)]
        send(part, DB.at[0, h], db_s.at[0, h], db_r.at[0, h], at_plane(1, p))
        send(part, DB.at[1, h], db_s.at[1, h], db_r.at[1, h], at_plane(-1, p))

    squares(lambda b: tok[b * TB:(b + 1) * TB, :].astype(F32), SQ)
    pl.semaphore_wait(barrier, NE - 1 + NT - 1)
    share(SQ, 0)
    send_h(0)

    r0 = rts[0:1, :]
    r1 = rts[1:2, :]
    eio = lax.broadcasted_iota(I32, (NE * 2, T), 0)
    oh0 = jnp.where(eio == r0, 1.0, 0.0)
    oh1 = jnp.where(eio == r1, 1.0, 0.0)
    up = jnp.where(
        lax.broadcasted_iota(I32, (T, T), 0) < lax.broadcasted_iota(I32, (T, T), 1), 1.0, 0.0
    ).astype(BF16)
    before = jnp.dot((oh0 + oh1).astype(BF16), up, preferred_element_type=F32)
    t0 = r0.astype(F32) * CAP + jnp.sum(oh0 * before, axis=0, keepdims=True)
    t1 = r1.astype(F32) * CAP + jnp.sum(oh1 * before, axis=0, keepdims=True)

    def near(k):
        wait(SQ.at[pl.ds(0, NT - 1)], sq_r.at[0])
        sub = lax.broadcasted_iota(I32, (8, T), 0)
        meta = jnp.where(sub == 0, t0, jnp.where(sub == 1, t1, scale_rows(SQ)))
        meta = jnp.where(sub == 2, rws[0:1, :], jnp.where(sub == 3, rws[1:2, :], meta))
        MT[...] = meta
        for slot, o in enumerate((1, -1, 2, -2)):
            send(MT, MR.at[slot], mt_s, mt_r.at[slot], at_plane(o, p))

    near(0)
    send_h(1)

    def pick(meta, at, xs, dst):
        rows = at.shape[0]
        s = meta[4:5, :]
        hit = (at == meta[0:1, :]) | (at == meta[1:2, :])
        scale = jnp.sum(jnp.where(hit, s, 0.0), axis=1, keepdims=True)
        sel = jnp.where(hit, 1.0, 0.0).astype(BF16)

        def cols(n, carry):
            cc = pl.ds(pl.multiple_of(n * CB, CB), CB)
            got = jnp.dot(sel[:, :HALF], xs[0][:, cc], preferred_element_type=F32)
            got = got + jnp.dot(sel[:, HALF:], xs[1][:, cc], preferred_element_type=F32)
            got = got * scale * ngain[0:1, cc]
            dst[:, :, cc] = got.astype(BF16).reshape(rows // G2, G2, CB)
            return carry

        lax.fori_loop(0, NB, cols, 0)

    def row_index(rows):
        return lax.broadcasted_iota(I32, (rows, T), 0)

    def stage_a(i):
        at = (row_index(RP) + z * RP).astype(F32)
        if i == 0:
            pick(MT, at, (tok.at[pl.ds(0, HALF)], tok.at[pl.ds(HALF, HALF)]), XS.at[0])
        else:
            wait_meta(i - 1)
            for h in range(2):
                wait_dense(i - 1, h)
            pick(MR.at[i - 1], at, (DB.at[i - 1, 0], DB.at[i - 1, 1]), XS.at[i])
        for j in range(1, NP):
            q = (p + j) % NP
            send(XS.at[i, q], XR.at[i, p], x_s.at[i], x_r.at[i], at_plane(0, q))
        XR[i, p] = XS[i, p]

    arrived = set()

    def wait_dense(k, h):
        if (k, h) not in arrived:
            arrived.add((k, h))
            wait(DB.at[k, h], db_r.at[k, h])

    def wait_meta(k):
        if k not in arrived:
            arrived.add(k)
            wait(MR.at[k], mt_r.at[k])

    def forward(h):
        for k in range(2):
            wait_dense(k, h)
            send(DB.at[k, h], DB.at[2 + k, h], db_s.at[2 + k, h], db_r.at[2 + k, h], at_plane(1 - 2 * k, p))

    def far(k):
        step = 1 - 2 * k
        for h in range(2):
            wait_dense(2 + k, h)
        wait_meta(2 + k)
        xs = (DB.at[2 + k, 0], DB.at[2 + k, 1])
        pick(MR.at[2 + k], (row_index(RP) + zz(step) * RP).astype(F32), xs, PS.at[k, pl.ds(0, NP)])
        for j in range(NP):
            q = (p + j) % NP
            send(PS.at[k, q], XR.at[5 + k, p], ps_s.at[k, 0], x_r.at[5 + k], at_plane(step, q))
        it = row_index(RP // 2)
        at = it // G2 * (2 * G2) + it % G2 + (zz(2 * step) * RP + k * G2)
        pick(MR.at[2 + k], at.astype(F32), xs, PS.at[k, pl.ds(NP, H)])
        for j in range(H):
            q = (p // 2 + j) % H
            send(PS.at[k, NP + q], XR.at[7, p], ps_s.at[k, 1], x_r.at[7], at_plane(2 * step, 2 * q + k))

    def stage_b(i):
        wait(XR.at[i, pl.ds(0, NP - 1)] if i <= 4 else XR.at[i], x_r.at[i])

        def one(j, carry):
            q = (y + 1 + j) % NT
            for m in range(2):
                rows = XR[i, :, m * CAP:(m + 1) * CAP, :].reshape(M, W)
                got = jnp.dot(rows, WGU[m, q], preferred_element_type=F32)
                GS[i, q, m] = got.astype(BF16)

            @pl.when(j < NT - 1)
            def _():
                send(GS.at[i, q], GR.at[i, y], g_s.at[i], g_r.at[i], {"tp": q})

            return carry

        lax.fori_loop(0, NT, one, 0)

    def stage_c(i):
        wait(GR.at[i, pl.ds(0, NT - 1)], g_r.at[i])
        for m in range(2):
            total = GS[i, y, m].astype(F32)
            for j in range(1, NT):
                total = total + GR[i, (y + j) % NT, m].astype(F32)
            gate = total[:, :FQ]
            HB[i, y, m] = (gate / (1.0 + jnp.exp(-gate)) * total[:, FQ:]).astype(BF16)
        for j in range(1, NT):
            send(HB.at[i, y], HB.at[i, y], h_s.at[i], h_r.at[i], tdev(j))

    def stage_d(i):
        wait(HB.at[i, pl.ds(0, NT - 1)], h_r.at[i])
        for m in range(2):
            hid = jnp.concatenate([HB[i, q, m] for q in range(NT)], axis=1)

            def cols(n, carry):
                cc = pl.ds(pl.multiple_of(n * CB, CB), CB)
                got = jnp.dot(hid, WD[m, :, cc], preferred_element_type=F32)
                OS[i, :, m * CAP:(m + 1) * CAP, cc] = got.astype(BF16).reshape(NP, CAP, CB)
                return carry

            lax.fori_loop(0, NB, cols, 0)
        if i == 0:
            for j in range(1, NP):
                q = (p + j) % NP
                send(OS.at[0, q], OR.at[p], o_s.at[0], o_r, at_plane(0, q))
            OR[p] = OS[0, p]
        elif i < 7:
            d = (i + 1) // 2
            side = (i + 1) % 2
            for j in range(1 if d == 1 else 0, NP):
                q = (p + j) % NP
                hop = (d - 1) * (2 * side - 1)
                send(OS.at[i, q], RV.at[side, (d - 1) * NP + p], o_s.at[i], rv_r.at[side, d - 1], at_plane(hop, q))
            if d == 1:
                RV[side, p] = OS[i, p]
        else:
            side = 1 - par
            for j in range(NP):
                q = (p + j) % NP
                send(OS.at[7, q], RV.at[side, 3 * NP + p // 2], o_s.at[7], rv_r.at[side, 3], at_plane(3 - 6 * par, q))

    def matrix(meta, at, b):
        bb = slice(b * TB, (b + 1) * TB)
        cols = [jnp.transpose(jnp.broadcast_to(meta[r:r + 1, bb], (128, TB))) for r in range(4)]
        out = []
        for a in at:
            out.append(jnp.where(a == cols[0], cols[2], 0.0) + jnp.where(a == cols[1], cols[3], 0.0))
        return jnp.concatenate(out, axis=1).astype(BF16)

    def lanes(base):
        return lax.broadcasted_iota(I32, (TB, 128), 1) + base

    def mats(k):
        own = [lanes(z * RP + c * 128).astype(F32) for c in range(RP // 128)]
        for b in range(T // TB):
            CO[b * TB:(b + 1) * TB, :] = matrix(MT, own, b)
        for side in range(2):
            wait_meta(side)
            s = 1 - 2 * side
            at = [lanes(zz(s * d) * RP + c * 128) for d in range(3) for c in range(RP // 128)]
            for c in range(RP // 256):
                it = lanes(c * 128)
                at.append(it // G2 * (2 * G2) + it % G2 + (zz(3 * s) * RP + (1 - side) * G2))
            at = [a.astype(F32) for a in at]
            for b in range(T // TB):
                CM[side, b * TB:(b + 1) * TB, :] = matrix(MR.at[side], at, b)

    def own_part(k):
        wait(OR.at[pl.ds(0, NP - 1)], o_r)

        def cols(n, carry):
            cc = pl.ds(pl.multiple_of(n * CB, CB), CB)
            ACC[n] = jnp.dot(CO[...], OR[:, :, cc].reshape(RP, CB), preferred_element_type=F32)
            return carry

        lax.fori_loop(0, NB, cols, 0)

    def relay(side):
        wait(RV.at[side, pl.ds(0, NP - 1)], rv_r.at[side, 0])
        for d in range(1, 3):
            wait(RV.at[side, pl.ds(d * NP, NP)], rv_r.at[side, d])
        wait(RV.at[side, pl.ds(3 * NP, H)], rv_r.at[side, 3])

        def cols(n, carry):
            cc = pl.ds(pl.multiple_of(n * CB, CB), CB)
            rows = RV[side, :, :, cc].reshape(CM.shape[2], CB)
            got = jnp.dot(CM[side], rows, preferred_element_type=F32)
            RS[side, n] = got.astype(BF16)
            send(RS.at[side, n], RD.at[side, n], rd_s.at[side, n], rd_r.at[side, n], at_plane(2 * side - 1, p))
            return carry

        lax.fori_loop(0, NB, cols, 0)

    stage_a(0)
    forward(0)
    wait(WGU, w_sem.at[0])
    wait(WD, w_sem.at[1])
    stage_b(0)
    stage_c(0)
    forward(1)
    stage_a(2)
    mats(0)
    stage_d(0)
    stage_a(1)
    stage_b(2)
    own_part(0)
    stage_c(2)
    stage_b(1)
    far(1)
    far(0)
    stage_d(2)
    stage_c(1)
    stage_a(3)
    stage_a(4)
    stage_d(1)
    stage_b(6)
    stage_b(5)
    stage_c(6)
    stage_c(5)
    stage_b(7)
    stage_b(3)
    stage_d(6)
    stage_d(5)
    stage_b(4)
    stage_c(7)
    stage_c(3)
    stage_c(4)
    stage_d(7)
    stage_d(3)
    stage_d(4)
    relay(1)
    relay(0)

    def finish(n, carry):
        for side in range(2):
            wait(RD.at[side, n], rd_r.at[side, n])
        ACC[n] = ACC[n] + RD[0, n].astype(F32) + RD[1, n].astype(F32)
        return carry

    lax.fori_loop(0, NB, finish, 0)

    def block(b):
        return jnp.concatenate([ACC[n, b * TB:(b + 1) * TB, :] for n in range(NB)], axis=1)

    squares(block, SQ2)
    share(SQ2, 1)
    wait(SQ2.at[pl.ds(0, NT - 1)], sq_r.at[1])
    final = scale_rows(SQ2)
    for b in range(T // TB):
        sc = jnp.transpose(jnp.broadcast_to(final[0:1, b * TB:(b + 1) * TB], (128, TB)))
        for c in range(W // 128):
            n, l = c * 128 // CB, c * 128 % CB
            v = ACC[n, b * TB:(b + 1) * TB, l:l + 128] * sc * fgain[0:1, c * 128:(c + 1) * 128]
            out[b * TB:(b + 1) * TB, c * 128:(c + 1) * 128] = v.astype(BF16)

    for k in range(2):
        wait(SQ.at[pl.ds(0, NT - 1)], sq_s.at[k])
        wait(PS.at[k, pl.ds(0, NP)], ps_s.at[k, 0])
        wait(PS.at[k, pl.ds(NP, H)], ps_s.at[k, 1])
        for n in range(NB):
            wait(RD.at[k, n], rd_s.at[k, n])
    wait(MR, mt_s)
    for k in range(4):
        for h in range(2):
            wait(DB.at[k, h], db_s.at[k, h])
    for i in range(NZ):
        if i <= 4:
            wait(XR.at[i, pl.ds(0, NP - 1)], x_s.at[i])
        wait(GR.at[i, pl.ds(0, NT - 1)], g_s.at[i])
        wait(HB.at[i, pl.ds(0, NT - 1)], h_s.at[i])
        wait(OS.at[i, pl.ds(0, NP - 1)] if i <= 2 else OS.at[i], o_s.at[i])


def cap_of(rows, planar):
    return 4 * rows // (NZ * planar * 2)


def body(tokens, routes, route_weights, norm_gain, gate_weight, up_weight, down_weight, final_gain):
    NT = lax.axis_size("tp")
    NP = lax.axis_size("ep") // NZ
    T, W = tokens.shape
    FF = gate_weight.shape[2]
    FQ = FF // NT
    CAP = cap_of(T, NP)
    G2 = 2 * CAP
    RP = NP * G2
    M = NP * CAP
    CB = 256 if W % 256 == 0 else 128
    NB = W // CB
    rows = (NP, G2, W)
    vm = pltpu.VMEM
    dma = pltpu.SemaphoreType.DMA
    scratch = [
        vm((4, 2, T // 2, W), BF16),
        vm((8, T), F32),
        vm((4, 8, T), F32),
        vm((5, *rows), BF16),
        vm((NZ, *rows), BF16),
        vm((2, NP + NP // 2, G2, W), BF16),
        vm((NZ, NT, 2, M, 2 * FQ), BF16),
        vm((NZ, NT, 2, M, 2 * FQ), BF16),
        vm((NZ, NT, 2, M, FQ), BF16),
        vm((NZ, *rows), BF16),
        vm(rows, BF16),
        vm((2, 3 * NP + NP // 2, G2, W), BF16),
        vm((T, RP), BF16),
        vm((2, T, 3 * RP + RP // 2), BF16),
        vm((2, NB, T, CB), BF16),
        vm((2, NB, T, CB), BF16),
        vm((NB, T, CB), F32),
        vm((2, NT, W, 2 * FQ), BF16),
        vm((2, FF, W), BF16),
        vm((NT, 8, T), F32),
        vm((NT, 8, T), F32),
        dma((2,)),
        dma((2,)), dma((2,)),
        dma, dma((4,)),
        dma((4, 2)), dma((4, 2)),
        dma((2, 2)),
        dma((5,)), dma((NZ,)),
        dma((NZ,)), dma((NZ,)),
        dma((NZ,)), dma((NZ,)),
        dma((NZ,)), dma,
        dma((2, 4)),
        dma((2, NB)), dma((2, NB)),
    ]
    v = pl.BlockSpec(memory_space=pltpu.VMEM)
    a = pl.BlockSpec(memory_space=pl.ANY)
    return pl.pallas_call(
        functools.partial(layer_kernel, NP, NT),
        out_shape=jax.ShapeDtypeStruct((T, W), BF16),
        in_specs=[v, v, v, v, v, a, a, a],
        out_specs=v,
        scratch_shapes=scratch,
        compiler_params=pltpu.CompilerParams(
            collective_id=0, has_side_effects=True, vmem_limit_bytes=67043328
        ),
    )(
        tokens, routes.T, route_weights.T, norm_gain[None], final_gain[None],
        gate_weight, up_weight, down_weight,
    )


def solution(mesh):
    in_specs = (
        P("ep", "tp"),
        P("ep", None),
        P("ep", None),
        P("tp"),
        P("ep", "tp", None),
        P("ep", "tp", None),
        P("ep", None, "tp"),
        P("tp"),
    )
    out_specs = P("ep", "tp")
    return jax.shard_map(body, mesh=mesh, in_specs=in_specs, out_specs=out_specs, check_vma=False)
```

```python
import functools

import jax
import jax.numpy as jnp
from jax import lax
from jax.experimental import pallas as pl
from jax.experimental.pallas import tpu as pltpu
from jax.sharding import PartitionSpec as P

EPSILON = 1e-06
NZ = 8
F32 = jnp.float32
BF16 = jnp.bfloat16
I32 = jnp.int32


def layer_kernel(
    NP, NT, tok, rts, rws, ngain, fgain, gw, uw, dw, out,
    DB, MT, MR, XS, XR, PS, GS, GR, HB, OS, OR, RV, RW, CO, CM, RS, RD, ACC, WGU, WD, SQ, SQ2, OUT,
    w_sem, sq_s, sq_r, mt_s, mt_r, db_s, db_r, ps_s, x_s, x_r, g_s, g_r, h_s, h_r,
    o_s, o_r, rv_r, rd_s, rd_r, out_s,
):
    T, W = tok.shape
    HALF = T // 2
    CAP = cap_of(T, NP)
    G2 = 2 * CAP
    RP = NP * G2
    M = NP * CAP
    FQ = WGU.shape[3] // 2
    CB = RS.shape[3]
    KA = 6 * NP * CAP
    NB = W // CB
    D = W * NT
    H = NP // 2
    NE = NZ * NP
    TB = min(128, T)
    ep = lax.axis_index("ep")
    y = lax.axis_index("tp")
    z = ep // NP
    p = ep % NP
    par = p % 2
    MESH = pl.DeviceIdType.MESH

    def zz(o):
        return (z + o + NZ) % NZ

    def at_plane(o, q):
        return {"ep": zz(o) * NP + q}

    def tdev(j):
        return {"tp": (y + j) % NT}

    def send(src, dst, ss, rs, dev):
        pltpu.make_async_remote_copy(
            src_ref=src, dst_ref=dst, send_sem=ss, recv_sem=rs, device_id=dev, device_id_type=MESH,
        ).start()

    def wait(ref, sem):
        pltpu.make_async_copy(ref, ref, sem).wait()

    barrier = pltpu.get_barrier_semaphore()

    def greet(j, carry):
        for o in (-3, -2, -1, 1, 2, 3):
            pl.semaphore_signal(barrier, inc=1, device_id=at_plane(o, j), device_id_type=MESH)
        return carry

    lax.fori_loop(0, NP, greet, 0)
    for j in range(1, NP):
        pl.semaphore_signal(barrier, inc=1, device_id=at_plane(0, (p + j) % NP), device_id_type=MESH)
    for j in range(1, NT):
        pl.semaphore_signal(barrier, inc=1, device_id=tdev(j), device_id_type=MESH)

    for m in range(2):
        for q in range(NT):
            cols = pl.ds(q * FQ, FQ)
            pltpu.make_async_copy(gw.at[m, :, cols], WGU.at[m, q, :, pl.ds(0, FQ)], w_sem.at[0]).start()
            pltpu.make_async_copy(uw.at[m, :, cols], WGU.at[m, q, :, pl.ds(FQ, FQ)], w_sem.at[0]).start()
    pltpu.make_async_copy(dw, WD, w_sem.at[1]).start()

    def squares(load, buf):
        for b in range(T // TB):
            v = load(b)
            s = jnp.sum(v * v, axis=1, keepdims=True)
            row = jnp.transpose(jnp.broadcast_to(s, (TB, 128)))
            buf[y, :, b * TB:(b + 1) * TB] = row[0:8, :]

    def share(buf, k):
        for j in range(1, NT):
            send(buf.at[y], buf.at[y], sq_s.at[k], sq_r.at[k], tdev(j))

    def scale_rows(buf):
        total = buf[0]
        for q in range(1, NT):
            total = total + buf[q]
        return lax.rsqrt(total / D + EPSILON)

    def send_h(h):
        part = tok.at[pl.ds(h * HALF, HALF)]
        send(part, DB.at[0, h], db_s.at[0, h], db_r.at[0, h], at_plane(1, p))
        send(part, DB.at[1, h], db_s.at[1, h], db_r.at[1, h], at_plane(-1, p))

    squares(lambda b: tok[b * TB:(b + 1) * TB, :].astype(F32), SQ)
    pl.semaphore_wait(barrier, 7 * NP - 1 + NT - 1)
    share(SQ, 0)
    send_h(0)

    r0 = rts[0:1, :]
    r1 = rts[1:2, :]
    eio = lax.broadcasted_iota(I32, (NE * 2, T), 0)
    oh0 = jnp.where(eio == r0, 1.0, 0.0)
    oh1 = jnp.where(eio == r1, 1.0, 0.0)
    up = jnp.where(
        lax.broadcasted_iota(I32, (T, T), 0) < lax.broadcasted_iota(I32, (T, T), 1), 1.0, 0.0
    ).astype(BF16)
    before = jnp.dot((oh0 + oh1).astype(BF16), up, preferred_element_type=F32)
    t0 = r0.astype(F32) * CAP + jnp.sum(oh0 * before, axis=0, keepdims=True)
    t1 = r1.astype(F32) * CAP + jnp.sum(oh1 * before, axis=0, keepdims=True)

    def near(k):
        wait(SQ.at[pl.ds(0, NT - 1)], sq_r.at[0])
        sub = lax.broadcasted_iota(I32, (8, T), 0)
        meta = jnp.where(sub == 0, t0, jnp.where(sub == 1, t1, scale_rows(SQ)))
        meta = jnp.where(sub == 2, rws[0:1, :], jnp.where(sub == 3, rws[1:2, :], meta))
        MT[...] = meta
        for slot, o in enumerate((1, -1, 2, -2)):
            send(MT, MR.at[slot], mt_s, mt_r.at[slot], at_plane(o, p))

    near(0)
    send_h(1)

    def pick(meta, at, xs, dst):
        rows = at.shape[0]
        s = meta[4:5, :]
        hit = (at == meta[0:1, :]) | (at == meta[1:2, :])
        scale = jnp.sum(jnp.where(hit, s, 0.0), axis=1, keepdims=True)
        sel = jnp.where(hit, 1.0, 0.0).astype(BF16)

        def cols(n, carry):
            cc = pl.ds(pl.multiple_of(n * CB, CB), CB)
            got = jnp.dot(sel[:, :HALF], xs[0][:, cc], preferred_element_type=F32)
            got = got + jnp.dot(sel[:, HALF:], xs[1][:, cc], preferred_element_type=F32)
            got = got * scale * ngain[0:1, cc]
            dst[:, :, :, cc] = got.astype(BF16).reshape(2, rows // G2, CAP, CB)
            return carry

        lax.fori_loop(0, NB, cols, 0)

    def row_index(rows, spread=1):
        r = lax.broadcasted_iota(I32, (rows, T), 0)
        half = rows // 2
        return (r % half) // CAP * (G2 * spread) + r // half * CAP + r % CAP

    def stage_a(i):
        at = (row_index(RP) + z * RP).astype(F32)
        if i == 0:
            pick(MT, at, (tok.at[pl.ds(0, HALF)], tok.at[pl.ds(HALF, HALF)]), XS.at[0])
        else:
            wait_meta(i - 1)
            for h in range(2):
                wait_dense(i - 1, h)
            pick(MR.at[i - 1], at, (DB.at[i - 1, 0], DB.at[i - 1, 1]), XS.at[i])
        for m in range(2):
            for j in range(1, NP):
                q = (p + j) % NP
                send(XS.at[i, m, q], XR.at[i, m, p], x_s.at[i, m], x_r.at[i, m], at_plane(0, q))
        for m in range(2):
            XR[i, m, p] = XS[i, m, p]

    arrived = set()

    def wait_dense(k, h):
        if (k, h) not in arrived:
            arrived.add((k, h))
            wait(DB.at[k, h], db_r.at[k, h])

    def wait_meta(k):
        if k not in arrived:
            arrived.add(k)
            wait(MR.at[k], mt_r.at[k])

    def forward(h):
        for k in range(2):
            wait_dense(k, h)
            send(DB.at[k, h], DB.at[2 + k, h], db_s.at[2 + k, h], db_r.at[2 + k, h], at_plane(1 - 2 * k, p))

    def far3(k):
        step = 1 - 2 * k
        for h in range(2):
            wait_dense(2 + k, h)
        wait_meta(2 + k)
        xs = (DB.at[2 + k, 0], DB.at[2 + k, 1])
        pick(MR.at[2 + k], (row_index(RP) + zz(step) * RP).astype(F32), xs, PS.at[k, :, pl.ds(0, NP)])
        for m in range(2):
            for j in range(NP):
                q = (p + j) % NP
                send(PS.at[k, m, q], XR.at[5 + k, m, p], ps_s.at[k, 0, m], x_r.at[5 + k, m], at_plane(step, q))

    def far4(k):
        step = 1 - 2 * k
        xs = (DB.at[2 + k, 0], DB.at[2 + k, 1])
        at = row_index(RP // 2, 2) + (zz(2 * step) * RP + k * G2)
        pick(MR.at[2 + k], at.astype(F32), xs, PS.at[k, :, pl.ds(NP, H)])
        for m in range(2):
            for j in range(H):
                q = (p // 2 + j) % H
                send(PS.at[k, m, NP + q], XR.at[7, m, p], ps_s.at[k, 1, m], x_r.at[7, m], at_plane(2 * step, 2 * q + k))

    def stage_b(i, m):
        wait(XR.at[i, m, pl.ds(0, NP - 1)] if i <= 4 else XR.at[i, m], x_r.at[i, m])

        def one(j, carry):
            q = (y + 1 + j) % NT
            rows = XR[i, m].reshape(M, W)
            got = jnp.dot(rows, WGU[m, q], preferred_element_type=F32)
            GS[i, m, q] = got.astype(BF16)

            @pl.when(j < NT - 1)
            def _():
                send(GS.at[i, m, q], GR.at[i, m, y], g_s.at[i, m], g_r.at[i, m], {"tp": q})

            return carry

        lax.fori_loop(0, NT, one, 0)

    def stage_c(i, m):
        wait(GR.at[i, m, pl.ds(0, NT - 1)], g_r.at[i, m])
        total = GS[i, m, y].astype(F32)
        for j in range(1, NT):
            total = total + GR[i, m, (y + j) % NT].astype(F32)
        gate = total[:, :FQ]
        HB[i, m, y] = (gate / (1.0 + jnp.exp(-gate)) * total[:, FQ:]).astype(BF16)
        for j in range(1, NT):
            send(HB.at[i, m, y], HB.at[i, m, y], h_s.at[i, m], h_r.at[i, m], tdev(j))

    def stage_d(i, m):
        wait(HB.at[i, m, pl.ds(0, NT - 1)], h_r.at[i, m])
        hid = jnp.concatenate([HB[i, m, q] for q in range(NT)], axis=1)

        def cols(n, carry):
            cc = pl.ds(pl.multiple_of(n * CB, CB), CB)
            got = jnp.dot(hid, WD[m, :, cc], preferred_element_type=F32)
            OS[i, m, :, :, cc] = got.astype(BF16).reshape(NP, CAP, CB)
            return carry

        lax.fori_loop(0, NB, cols, 0)
        if i == 0:
            for j in range(1, NP):
                q = (p + j) % NP
                send(OS.at[0, m, q], OR.at[m, p], o_s.at[0, m], o_r.at[m], at_plane(0, q))
            OR[m, p] = OS[0, m, p]
        elif i < 7:
            d = (i + 1) // 2
            side = (i + 1) % 2
            for j in range(1 if d == 1 else 0, NP):
                q = (p + j) % NP
                hop = (d - 1) * (2 * side - 1)
                send(
                    OS.at[i, m, q], RV.at[side, m, (d - 1) * NP + p], o_s.at[i, m],
                    rv_r.at[side, d - 1, m], at_plane(hop, q),
                )
            if d == 1:
                RV[side, m, p] = OS[i, m, p]
        else:
            side = 1 - par
            for j in range(NP):
                q = (p + j) % NP
                send(
                    OS.at[7, m, q], RW.at[side, m, p // 2], o_s.at[7, m],
                    rv_r.at[side, 3, m], at_plane(3 - 6 * par, q),
                )

    def matrix(meta, at, b):
        bb = slice(b * TB, (b + 1) * TB)
        cols = [jnp.transpose(jnp.broadcast_to(meta[r:r + 1, bb], (128, TB))) for r in range(4)]
        out = []
        for a in at:
            out.append(jnp.where(a == cols[0], cols[2], 0.0) + jnp.where(a == cols[1], cols[3], 0.0))
        return jnp.concatenate(out, axis=1).astype(BF16)

    def lanes(base):
        return lax.broadcasted_iota(I32, (TB, 128), 1) + base

    def mats(k):
        def place(col, groups, step):
            m = col // (groups * CAP)
            r = col % (groups * CAP)
            return r // CAP % NP * (G2 * step) + m * CAP + r % CAP

        own = [(z * RP + place(lanes(c * 128), NP, 1)).astype(F32) for c in range(RP // 128)]
        for b in range(T // TB):
            CO[b * TB:(b + 1) * TB, :] = matrix(MT, own, b)
        for side in range(2):
            wait_meta(side)
            s = 1 - 2 * side
            at = []
            for c in range(KA // 128):
                col = lanes(c * 128)
                d = col % (KA // 2) // (NP * CAP)
                plane = jnp.where(d == 0, z, jnp.where(d == 1, zz(s), zz(2 * s)))
                at.append((plane * RP + place(col, 3 * NP, 1)).astype(F32))
            for c in range(RP // 256):
                col = place(lanes(c * 128), H, 2)
                at.append((col + (zz(3 * s) * RP + (1 - side) * G2)).astype(F32))
            for b in range(T // TB):
                CM[side, b * TB:(b + 1) * TB, :] = matrix(MR.at[side], at, b)

    def own_part(k):
        for m in range(2):
            wait(OR.at[m, pl.ds(0, NP - 1)], o_r.at[m])

        def cols(n, carry):
            cc = pl.ds(pl.multiple_of(n * CB, CB), CB)
            ACC[n] = jnp.dot(CO[...], OR[:, :, :, cc].reshape(RP, CB), preferred_element_type=F32)
            return carry

        lax.fori_loop(0, NB, cols, 0)

    def relay(k):
        for m in range(2):
            for side in range(2):
                wait(RV.at[side, m, pl.ds(0, NP - 1)], rv_r.at[side, 0, m])
                for d in range(1, 3):
                    wait(RV.at[side, m, pl.ds(d * NP, NP)], rv_r.at[side, d, m])
                wait(RW.at[side, m], rv_r.at[side, 3, m])

        def cols(n, carry):
            cc = pl.ds(pl.multiple_of(n * CB, CB), CB)
            for side in range(2):
                rows = RV[side, :, :, :, cc].reshape(KA, CB)
                more = RW[side, :, :, :, cc].reshape(RP // 2, CB)
                got = jnp.dot(CM[side, :, :KA], rows, preferred_element_type=F32)
                got = got + jnp.dot(CM[side, :, KA:], more, preferred_element_type=F32)
                RS[side, n] = got.astype(BF16)
                send(RS.at[side, n], RD.at[side, n], rd_s.at[side, n], rd_r.at[side, n], at_plane(2 * side - 1, p))
            return carry

        lax.fori_loop(0, NB, cols, 0)

    stage_a(0)
    wait(WGU, w_sem.at[0])
    stage_b(0, 0)
    stage_b(0, 1)
    forward(0)
    stage_c(0, 0)
    stage_c(0, 1)
    wait(WD, w_sem.at[1])
    stage_d(0, 0)
    stage_a(2)
    forward(1)
    stage_b(2, 0)
    stage_a(1)
    stage_b(2, 1)
    stage_d(0, 1)
    stage_c(2, 1)
    stage_b(1, 1)
    stage_b(1, 0)
    stage_c(2, 0)
    far3(0)
    far3(1)
    stage_a(3)
    far4(1)
    stage_c(1, 1)
    stage_c(1, 0)
    far4(0)
    stage_a(4)
    stage_b(5, 0)
    stage_d(1, 0)
    stage_b(6, 0)
    stage_d(1, 1)
    stage_d(2, 1)
    stage_c(5, 0)
    stage_c(6, 0)
    stage_b(6, 1)
    stage_b(5, 1)
    stage_d(2, 0)
    stage_b(3, 0)
    stage_d(5, 0)
    stage_d(6, 0)
    stage_c(6, 1)
    stage_c(5, 1)
    stage_b(7, 0)
    stage_c(3, 0)
    stage_b(3, 1)
    stage_b(7, 1)
    stage_d(6, 1)
    stage_d(5, 1)
    mats(0)
    own_part(0)
    stage_c(7, 0)
    stage_b(4, 0)
    stage_c(3, 1)
    stage_c(7, 1)
    stage_b(4, 1)
    stage_d(7, 0)
    stage_d(3, 1)
    stage_c(4, 0)
    stage_d(7, 1)
    stage_c(4, 1)
    stage_d(4, 1)
    stage_d(4, 0)
    stage_d(3, 0)
    relay(0)

    def finish(n, carry):
        for side in range(2):
            wait(RD.at[side, n], rd_r.at[side, n])
        ACC[n] = ACC[n] + RD[0, n].astype(F32) + RD[1, n].astype(F32)
        return carry

    lax.fori_loop(0, NB, finish, 0)

    def block(b):
        return jnp.concatenate([ACC[n, b * TB:(b + 1) * TB, :] for n in range(NB)], axis=1)

    squares(block, SQ2)
    share(SQ2, 1)
    wait(SQ2.at[pl.ds(0, NT - 1)], sq_r.at[1])
    final = scale_rows(SQ2)
    for b in range(T // TB):
        sc = jnp.transpose(jnp.broadcast_to(final[0:1, b * TB:(b + 1) * TB], (128, TB)))
        for c in range(W // 128):
            n, l = c * 128 // CB, c * 128 % CB
            v = ACC[n, b * TB:(b + 1) * TB, l:l + 128] * sc * fgain[0:1, c * 128:(c + 1) * 128]
            OUT[b * TB:(b + 1) * TB, c * 128:(c + 1) * 128] = v.astype(BF16)
        pltpu.make_async_copy(OUT.at[pl.ds(b * TB, TB)], out.at[pl.ds(b * TB, TB)], out_s).start()

    for k in range(2):
        wait(SQ.at[pl.ds(0, NT - 1)], sq_s.at[k])
        for m in range(2):
            wait(PS.at[k, m, pl.ds(0, NP)], ps_s.at[k, 0, m])
            wait(PS.at[k, m, pl.ds(NP, H)], ps_s.at[k, 1, m])
        for n in range(NB):
            wait(RD.at[k, n], rd_s.at[k, n])
    wait(MR, mt_s)
    for k in range(4):
        for h in range(2):
            wait(DB.at[k, h], db_s.at[k, h])
    for i in range(NZ):
        for m in range(2):
            if i <= 4:
                wait(XR.at[i, m, pl.ds(0, NP - 1)], x_s.at[i, m])
            wait(GR.at[i, m, pl.ds(0, NT - 1)], g_s.at[i, m])
            wait(HB.at[i, m, pl.ds(0, NT - 1)], h_s.at[i, m])
            wait(OS.at[i, m, pl.ds(0, NP - 1)] if i <= 2 else OS.at[i, m], o_s.at[i, m])
    wait(OUT, out_s)


def cap_of(rows, planar):
    return 4 * rows // (NZ * planar * 2)


def body(tokens, routes, route_weights, norm_gain, gate_weight, up_weight, down_weight, final_gain):
    NT = lax.axis_size("tp")
    NP = lax.axis_size("ep") // NZ
    T, W = tokens.shape
    FF = gate_weight.shape[2]
    FQ = FF // NT
    CAP = cap_of(T, NP)
    G2 = 2 * CAP
    RP = NP * G2
    M = NP * CAP
    CB = 256 if W % 256 == 0 else 128
    NB = W // CB
    rows = (2, NP, CAP, W)
    vm = pltpu.VMEM
    dma = pltpu.SemaphoreType.DMA
    scratch = [
        vm((4, 2, T // 2, W), BF16),
        vm((8, T), F32),
        vm((4, 8, T), F32),
        vm((5, *rows), BF16),
        vm((NZ, *rows), BF16),
        vm((2, 2, NP + NP // 2, CAP, W), BF16),
        vm((NZ, 2, NT, M, 2 * FQ), BF16),
        vm((NZ, 2, NT, M, 2 * FQ), BF16),
        vm((NZ, 2, NT, M, FQ), BF16),
        vm((NZ, *rows), BF16),
        vm(rows, BF16),
        vm((2, 2, 3 * NP, CAP, W), BF16),
        vm((2, 2, NP // 2, CAP, W), BF16),
        vm((T, RP), BF16),
        vm((2, T, 3 * RP + RP // 2), BF16),
        vm((2, NB, T, CB), BF16),
        vm((2, NB, T, CB), BF16),
        vm((NB, T, CB), F32),
        vm((2, NT, W, 2 * FQ), BF16),
        vm((2, FF, W), BF16),
        vm((NT, 8, T), F32),
        vm((NT, 8, T), F32),
        vm((T, W), BF16),
        dma((2,)),
        dma((2,)), dma((2,)),
        dma, dma((4,)),
        dma((4, 2)), dma((4, 2)),
        dma((2, 2, 2)),
        dma((5, 2)), dma((NZ, 2)),
        dma((NZ, 2)), dma((NZ, 2)),
        dma((NZ, 2)), dma((NZ, 2)),
        dma((NZ, 2)), dma((2,)),
        dma((2, 4, 2)),
        dma((2, NB)), dma((2, NB)),
        dma,
    ]
    v = pl.BlockSpec(memory_space=pltpu.VMEM)
    a = pl.BlockSpec(memory_space=pl.ANY)
    return pl.pallas_call(
        functools.partial(layer_kernel, NP, NT),
        out_shape=jax.ShapeDtypeStruct((T, W), BF16),
        in_specs=[v, v, v, v, v, a, a, a],
        out_specs=a,
        scratch_shapes=scratch,
        compiler_params=pltpu.CompilerParams(
            collective_id=0, has_side_effects=True, vmem_limit_bytes=67043328
        ),
    )(
        tokens, routes.T, route_weights.T, norm_gain[None], final_gain[None],
        gate_weight, up_weight, down_weight,
    )


def solution(mesh):
    in_specs = (
        P("ep", "tp"),
        P("ep", None),
        P("ep", None),
        P("tp"),
        P("ep", "tp", None),
        P("ep", "tp", None),
        P("ep", None, "tp"),
        P("tp"),
    )
    out_specs = P("ep", "tp")
    return jax.shard_map(body, mesh=mesh, in_specs=in_specs, out_specs=out_specs, check_vma=False)
```

```python
import functools

import jax
import jax.numpy as jnp
from jax import lax
from jax.experimental import pallas as pl
from jax.experimental.pallas import tpu as pltpu
from jax.sharding import PartitionSpec as P

EPSILON = 1e-06
NZ = 8
F32 = jnp.float32
BF16 = jnp.bfloat16
I32 = jnp.int32


def layer_kernel(
    NP, NT, tok_hbm, rts, rws, ngain, fgain, gw, uw, dw, out,
    DB, MT, MR, XS, XR, PS, GS, GR, HB, OS, OR, RV, RW, CO, CM, RS, RD, ACC, WGU, WD, SQ, SQ2, OUT, tok, tok_s,
    w_sem, sq_s, sq_r, mt_s, mt_r, db_s, db_r, ps_s, x_s, x_r, g_s, g_r, h_s, h_r,
    o_s, o_r, rv_r, rb_r, ob_s, rd_s, rd_r, out_s,
):
    T, W = tok.shape
    HALF = T // 2
    CAP = cap_of(T, NP)
    G2 = 2 * CAP
    RP = NP * G2
    M = NP * CAP
    FQ = WGU.shape[3] // 2
    CB = RS.shape[3]
    KA = 6 * NP * CAP
    NB = W // CB
    D = W * NT
    H = NP // 2
    NE = NZ * NP
    TB = min(128, T)
    ep = lax.axis_index("ep")
    y = lax.axis_index("tp")
    z = ep // NP
    p = ep % NP
    par = p % 2
    MESH = pl.DeviceIdType.MESH

    def zz(o):
        return (z + o + NZ) % NZ

    def at_plane(o, q):
        return {"ep": zz(o) * NP + q}

    def tdev(j):
        return {"tp": (y + j) % NT}

    def send(src, dst, ss, rs, dev):
        pltpu.make_async_remote_copy(
            src_ref=src, dst_ref=dst, send_sem=ss, recv_sem=rs, device_id=dev, device_id_type=MESH,
        ).start()

    def wait(ref, sem):
        pltpu.make_async_copy(ref, ref, sem).wait()

    barrier = pltpu.get_barrier_semaphore()

    def greet(j, carry):
        for o in (-3, -2, -1, 1, 2, 3):
            pl.semaphore_signal(barrier, inc=1, device_id=at_plane(o, j), device_id_type=MESH)
        return carry

    lax.fori_loop(0, NP, greet, 0)
    for j in range(1, NP):
        pl.semaphore_signal(barrier, inc=1, device_id=at_plane(0, (p + j) % NP), device_id_type=MESH)
    for j in range(1, NT):
        pl.semaphore_signal(barrier, inc=1, device_id=tdev(j), device_id_type=MESH)

    pltpu.make_async_copy(tok_hbm, tok, tok_s).start()
    wait(tok, tok_s)
    for m in range(2):
        for q in range(NT):
            cols = pl.ds(q * FQ, FQ)
            pltpu.make_async_copy(gw.at[m, :, cols], WGU.at[m, q, :, pl.ds(0, FQ)], w_sem.at[0]).start()
            pltpu.make_async_copy(uw.at[m, :, cols], WGU.at[m, q, :, pl.ds(FQ, FQ)], w_sem.at[0]).start()
    pltpu.make_async_copy(dw, WD, w_sem.at[1]).start()

    def squares(load, buf):
        for b in range(T // TB):
            v = load(b)
            s = jnp.sum(v * v, axis=1, keepdims=True)
            row = jnp.transpose(jnp.broadcast_to(s, (TB, 128)))
            buf[y, :, b * TB:(b + 1) * TB] = row[0:8, :]

    def share(buf, k):
        for j in range(1, NT):
            send(buf.at[y], buf.at[y], sq_s.at[k], sq_r.at[k], tdev(j))

    def scale_rows(buf):
        total = buf[0]
        for q in range(1, NT):
            total = total + buf[q]
        return lax.rsqrt(total / D + EPSILON)

    def send_h(h):
        part = tok.at[pl.ds(h * HALF, HALF)]
        send(part, DB.at[0, h], db_s.at[0, h], db_r.at[0, h], at_plane(1, p))
        send(part, DB.at[1, h], db_s.at[1, h], db_r.at[1, h], at_plane(-1, p))

    pl.semaphore_wait(barrier, 7 * NP - 1 + NT - 1)
    send_h(0)
    squares(lambda b: tok[b * TB:(b + 1) * TB, :].astype(F32), SQ)
    share(SQ, 0)

    r0 = rts[0:1, :]
    r1 = rts[1:2, :]
    eio = lax.broadcasted_iota(I32, (NE * 2, T), 0)
    oh0 = jnp.where(eio == r0, 1.0, 0.0)
    oh1 = jnp.where(eio == r1, 1.0, 0.0)
    up = jnp.where(
        lax.broadcasted_iota(I32, (T, T), 0) < lax.broadcasted_iota(I32, (T, T), 1), 1.0, 0.0
    ).astype(BF16)
    before = jnp.dot((oh0 + oh1).astype(BF16), up, preferred_element_type=F32)
    t0 = r0.astype(F32) * CAP + jnp.sum(oh0 * before, axis=0, keepdims=True)
    t1 = r1.astype(F32) * CAP + jnp.sum(oh1 * before, axis=0, keepdims=True)

    def near(k):
        wait(SQ.at[pl.ds(0, NT - 1)], sq_r.at[0])
        sub = lax.broadcasted_iota(I32, (8, T), 0)
        meta = jnp.where(sub == 0, t0, jnp.where(sub == 1, t1, scale_rows(SQ)))
        meta = jnp.where(sub == 2, rws[0:1, :], jnp.where(sub == 3, rws[1:2, :], meta))
        MT[...] = meta
        for slot, o in enumerate((1, -1, 2, -2)):
            send(MT, MR.at[slot], mt_s, mt_r.at[slot], at_plane(o, p))

    near(0)
    send_h(1)

    def pick(meta, at, xs, dst):
        rows = at.shape[0]
        s = meta[4:5, :]
        hit = (at == meta[0:1, :]) | (at == meta[1:2, :])
        scale = jnp.sum(jnp.where(hit, s, 0.0), axis=1, keepdims=True)
        sel = jnp.where(hit, 1.0, 0.0).astype(BF16)

        def cols(n, carry):
            cc = pl.ds(pl.multiple_of(n * CB, CB), CB)
            got = jnp.dot(sel[:, :HALF], xs[0][:, cc], preferred_element_type=F32)
            got = got + jnp.dot(sel[:, HALF:], xs[1][:, cc], preferred_element_type=F32)
            got = got * scale * ngain[0:1, cc]
            dst[:, :, :, cc] = got.astype(BF16).reshape(2, rows // G2, CAP, CB)
            return carry

        lax.fori_loop(0, NB, cols, 0)

    def row_index(rows, spread=1):
        r = lax.broadcasted_iota(I32, (rows, T), 0)
        half = rows // 2
        return (r % half) // CAP * (G2 * spread) + r // half * CAP + r % CAP

    def stage_a(i):
        at = (row_index(RP) + z * RP).astype(F32)
        if i == 0:
            pick(MT, at, (tok.at[pl.ds(0, HALF)], tok.at[pl.ds(HALF, HALF)]), XS.at[0])
        else:
            wait_meta(i - 1)
            for h in range(2):
                wait_dense(i - 1, h)
            pick(MR.at[i - 1], at, (DB.at[i - 1, 0], DB.at[i - 1, 1]), XS.at[i])
        for m in range(2):
            for j in range(1, NP):
                q = (p + j) % NP
                send(XS.at[i, m, q], XR.at[i, m, p], x_s.at[i, m], x_r.at[i, m], at_plane(0, q))
        for m in range(2):
            XR[i, m, p] = XS[i, m, p]

    arrived = set()

    def wait_dense(k, h):
        if (k, h) not in arrived:
            arrived.add((k, h))
            wait(DB.at[k, h], db_r.at[k, h])

    def wait_meta(k):
        if k not in arrived:
            arrived.add(k)
            wait(MR.at[k], mt_r.at[k])

    def forward(h):
        for k in range(2):
            wait_dense(k, h)
            send(DB.at[k, h], DB.at[2 + k, h], db_s.at[2 + k, h], db_r.at[2 + k, h], at_plane(1 - 2 * k, p))

    def far3(k):
        step = 1 - 2 * k
        for h in range(2):
            wait_dense(2 + k, h)
        wait_meta(2 + k)
        xs = (DB.at[2 + k, 0], DB.at[2 + k, 1])
        pick(MR.at[2 + k], (row_index(RP) + zz(step) * RP).astype(F32), xs, PS.at[k, :, pl.ds(0, NP)])
        for m in range(2):
            for j in range(NP):
                q = (p + j) % NP
                send(PS.at[k, m, q], XR.at[5 + k, m, p], ps_s.at[k, 0, m], x_r.at[5 + k, m], at_plane(step, q))

    def far4(k):
        step = 1 - 2 * k
        xs = (DB.at[2 + k, 0], DB.at[2 + k, 1])
        at = row_index(RP // 2, 2) + (zz(2 * step) * RP + k * G2)
        pick(MR.at[2 + k], at.astype(F32), xs, PS.at[k, :, pl.ds(NP, H)])
        for m in range(2):
            for j in range(H):
                q = (p // 2 + j) % H
                send(PS.at[k, m, NP + q], XR.at[7, m, p], ps_s.at[k, 1, m], x_r.at[7, m], at_plane(2 * step, 2 * q + k))

    def stage_b(i, m):
        wait(XR.at[i, m, pl.ds(0, NP - 1)] if i <= 4 else XR.at[i, m], x_r.at[i, m])

        def one(j, carry):
            q = (y + 1 + j) % NT
            rows = XR[i, m].reshape(M, W)
            got = jnp.dot(rows, WGU[m, q], preferred_element_type=F32)
            GS[i, m, q] = got.astype(BF16)

            @pl.when(j < NT - 1)
            def _():
                send(GS.at[i, m, q], GR.at[i, m, y], g_s.at[i, m], g_r.at[i, m], {"tp": q})

            return carry

        lax.fori_loop(0, NT, one, 0)

    def stage_c(i, m):
        wait(GR.at[i, m, pl.ds(0, NT - 1)], g_r.at[i, m])
        total = GS[i, m, y].astype(F32)
        for j in range(1, NT):
            total = total + GR[i, m, (y + j) % NT].astype(F32)
        gate = total[:, :FQ]
        HB[i, m, y] = (gate / (1.0 + jnp.exp(-gate)) * total[:, FQ:]).astype(BF16)
        for j in range(1, NT):
            send(HB.at[i, m, y], HB.at[i, m, y], h_s.at[i, m], h_r.at[i, m], tdev(j))

    def stage_d(i, m):
        wait(HB.at[i, m, pl.ds(0, NT - 1)], h_r.at[i, m])
        hid = jnp.concatenate([HB[i, m, q] for q in range(NT)], axis=1)

        def cols(n, carry):
            cc = pl.ds(pl.multiple_of(n * CB, CB), CB)
            got = jnp.dot(hid, WD[m, :, cc], preferred_element_type=F32)
            OS[i, m, :, :, cc] = got.astype(BF16).reshape(NP, CAP, CB)
            return carry

        lax.fori_loop(0, NB, cols, 0)
        if i == 0:
            for j in range(1, NP):
                q = (p + j) % NP
                send(OS.at[0, m, q], OR.at[m, p], o_s.at[0, m], o_r.at[m], at_plane(0, q))
            OR[m, p] = OS[0, m, p]
        else:
            returns(i, m, 0 if i in LATE else None)

    LATE = (3, 4, 7)

    def returns(i, m, part):
        cc = pl.ds(0, W) if part is None else pl.ds(part * (W // 2), W // 2)
        d = (i + 1) // 2
        ssem = o_s.at[i, m] if part != 1 else ob_s.at[LATE.index(i), m]
        for j in range(1 if d == 1 else 0, NP):
            q = (p + j) % NP
            if i < 7:
                side = (i + 1) % 2
                there = at_plane((d - 1) * (2 * side - 1), q)
                dst = RV.at[side, m, (d - 1) * NP + p, :, cc]
            else:
                side = 1 - par
                there = at_plane(3 - 6 * par, q)
                dst = RW.at[side, m, p // 2, :, cc]
            rsem = rv_r.at[side, d - 1, m] if part != 1 else rb_r.at[side, d // 4, m]
            send(OS.at[i, m, q, :, cc], dst, ssem, rsem, there)
        if d == 1:
            RV[side, m, p] = OS[i, m, p]

    def matrix(meta, at, b):
        bb = slice(b * TB, (b + 1) * TB)
        cols = [jnp.transpose(jnp.broadcast_to(meta[r:r + 1, bb], (128, TB))) for r in range(4)]
        out = []
        for a in at:
            out.append(jnp.where(a == cols[0], cols[2], 0.0) + jnp.where(a == cols[1], cols[3], 0.0))
        return jnp.concatenate(out, axis=1).astype(BF16)

    def lanes(base):
        return lax.broadcasted_iota(I32, (TB, 128), 1) + base

    def mats(k):
        def place(col, groups, step):
            m = col // (groups * CAP)
            r = col % (groups * CAP)
            return r // CAP % NP * (G2 * step) + m * CAP + r % CAP

        own = [(z * RP + place(lanes(c * 128), NP, 1)).astype(F32) for c in range(RP // 128)]
        for b in range(T // TB):
            CO[b * TB:(b + 1) * TB, :] = matrix(MT, own, b)
        for side in range(2):
            wait_meta(side)
            s = 1 - 2 * side
            at = []
            for c in range(KA // 128):
                col = lanes(c * 128)
                d = col % (KA // 2) // (NP * CAP)
                plane = jnp.where(d == 0, z, jnp.where(d == 1, zz(s), zz(2 * s)))
                at.append((plane * RP + place(col, 3 * NP, 1)).astype(F32))
            for c in range(RP // 256):
                col = place(lanes(c * 128), H, 2)
                at.append((col + (zz(3 * s) * RP + (1 - side) * G2)).astype(F32))
            for b in range(T // TB):
                CM[side, b * TB:(b + 1) * TB, :] = matrix(MR.at[side], at, b)

    def own_part(k):
        for m in range(2):
            wait(OR.at[m, pl.ds(0, NP - 1)], o_r.at[m])

        def cols(n, carry):
            cc = pl.ds(pl.multiple_of(n * CB, CB), CB)
            ACC[n] = jnp.dot(CO[...], OR[:, :, :, cc].reshape(RP, CB), preferred_element_type=F32)
            return carry

        lax.fori_loop(0, NB, cols, 0)

    def relay(k):
        cc = pl.ds(k * (W // 2), W // 2)
        for m in range(2):
            for side in range(2):
                if k == 0:
                    wait(RV.at[side, m, pl.ds(0, NP - 1)], rv_r.at[side, 0, m])
                    wait(RV.at[side, m, pl.ds(2 * NP, NP)], rv_r.at[side, 2, m])
                wait(RV.at[side, m, pl.ds(NP, NP), :, cc], (rb_r if k else rv_r).at[side, 1 - k, m])
                wait(RW.at[side, m, :, :, cc], rb_r.at[side, 1, m] if k else rv_r.at[side, 3, m])

        def cols(n, carry):
            cc = pl.ds(pl.multiple_of(n * CB, CB), CB)
            for side in range(2):
                rows = RV[side, :, :, :, cc].reshape(KA, CB)
                more = RW[side, :, :, :, cc].reshape(RP // 2, CB)
                got = jnp.dot(CM[side, :, :KA], rows, preferred_element_type=F32)
                got = got + jnp.dot(CM[side, :, KA:], more, preferred_element_type=F32)
                RS[side, n] = got.astype(BF16)
                send(RS.at[side, n], RD.at[side, n], rd_s.at[side, n], rd_r.at[side, n], at_plane(2 * side - 1, p))
            return carry

        lax.fori_loop(k * NB // 2, (k + 1) * NB // 2, cols, 0)

    stage_a(0)
    wait(WGU, w_sem.at[0])
    stage_b(0, 0)
    stage_c(0, 0)
    forward(0)
    stage_b(0, 1)
    wait(WD, w_sem.at[1])
    stage_d(0, 0)
    stage_a(2)
    stage_c(0, 1)
    forward(1)
    stage_a(1)
    stage_b(2, 0)
    stage_b(2, 1)
    stage_d(0, 1)
    stage_b(1, 1)
    mats(0)
    stage_c(2, 0)
    stage_c(2, 1)
    stage_b(1, 0)
    far3(0)
    far3(1)
    far4(0)
    stage_c(1, 0)
    far4(1)
    stage_c(1, 1)
    stage_b(5, 0)
    stage_b(6, 0)
    stage_a(4)
    stage_c(5, 0)
    stage_a(3)
    stage_c(6, 0)
    stage_b(5, 1)
    stage_d(5, 0)
    stage_b(6, 1)
    stage_b(7, 0)
    stage_d(6, 0)
    stage_c(5, 1)
    stage_c(6, 1)
    stage_b(4, 0)
    stage_b(7, 1)
    stage_b(4, 1)
    stage_d(5, 1)
    stage_d(6, 1)
    stage_c(7, 0)
    stage_b(3, 1)
    stage_d(2, 0)
    stage_d(1, 0)
    stage_d(7, 0)
    returns(7, 0, 1)
    stage_c(4, 1)
    stage_c(4, 0)
    stage_d(2, 1)
    stage_c(3, 1)
    stage_c(7, 1)
    stage_b(3, 0)
    stage_d(4, 0)
    own_part(0)
    stage_d(3, 1)
    stage_d(7, 1)
    stage_d(4, 1)
    returns(7, 1, 1)
    stage_d(1, 1)
    stage_c(3, 0)
    stage_d(3, 0)
    returns(3, 1, 1)
    returns(4, 0, 1)
    returns(4, 1, 1)
    returns(3, 0, 1)
    relay(0)
    relay(1)

    def finish(n, carry):
        for side in range(2):
            wait(RD.at[side, n], rd_r.at[side, n])
        ACC[n] = ACC[n] + RD[0, n].astype(F32) + RD[1, n].astype(F32)
        return carry

    lax.fori_loop(0, NB, finish, 0)

    def block(b):
        return jnp.concatenate([ACC[n, b * TB:(b + 1) * TB, :] for n in range(NB)], axis=1)

    squares(block, SQ2)
    share(SQ2, 1)
    wait(SQ2.at[pl.ds(0, NT - 1)], sq_r.at[1])
    final = scale_rows(SQ2)
    for b in range(T // TB):
        sc = jnp.transpose(jnp.broadcast_to(final[0:1, b * TB:(b + 1) * TB], (128, TB)))
        for c in range(W // 128):
            n, l = c * 128 // CB, c * 128 % CB
            v = ACC[n, b * TB:(b + 1) * TB, l:l + 128] * sc * fgain[0:1, c * 128:(c + 1) * 128]
            OUT[b * TB:(b + 1) * TB, c * 128:(c + 1) * 128] = v.astype(BF16)
        pltpu.make_async_copy(OUT.at[pl.ds(b * TB, TB)], out.at[pl.ds(b * TB, TB)], out_s).start()

    for k in range(2):
        wait(SQ.at[pl.ds(0, NT - 1)], sq_s.at[k])
        for m in range(2):
            wait(PS.at[k, m, pl.ds(0, NP)], ps_s.at[k, 0, m])
            wait(PS.at[k, m, pl.ds(NP, H)], ps_s.at[k, 1, m])
        for n in range(NB):
            wait(RD.at[k, n], rd_s.at[k, n])
    wait(MR, mt_s)
    for k in range(4):
        for h in range(2):
            wait(DB.at[k, h], db_s.at[k, h])
    for i in range(NZ):
        for m in range(2):
            if i <= 4:
                wait(XR.at[i, m, pl.ds(0, NP - 1)], x_s.at[i, m])
            wait(GR.at[i, m, pl.ds(0, NT - 1)], g_s.at[i, m])
            wait(HB.at[i, m, pl.ds(0, NT - 1)], h_s.at[i, m])
            if i in LATE:
                for k, sem in enumerate((o_s.at[i, m], ob_s.at[LATE.index(i), m])):
                    wait(OS.at[i, m, :, :, pl.ds(k * (W // 2), W // 2)], sem)
            else:
                wait(OS.at[i, m, pl.ds(0, NP - 1)] if i <= 2 else OS.at[i, m], o_s.at[i, m])
    wait(OUT, out_s)


def cap_of(rows, planar):
    return 4 * rows // (NZ * planar * 2)


def body(tokens, routes, route_weights, norm_gain, gate_weight, up_weight, down_weight, final_gain):
    NT = lax.axis_size("tp")
    NP = lax.axis_size("ep") // NZ
    T, W = tokens.shape
    FF = gate_weight.shape[2]
    FQ = FF // NT
    CAP = cap_of(T, NP)
    G2 = 2 * CAP
    RP = NP * G2
    M = NP * CAP
    CB = 256 if W % 256 == 0 else 128
    NB = W // CB
    rows = (2, NP, CAP, W)
    vm = pltpu.VMEM
    dma = pltpu.SemaphoreType.DMA
    scratch = [
        vm((4, 2, T // 2, W), BF16),
        vm((8, T), F32),
        vm((4, 8, T), F32),
        vm((5, *rows), BF16),
        vm((NZ, *rows), BF16),
        vm((2, 2, NP + NP // 2, CAP, W), BF16),
        vm((NZ, 2, NT, M, 2 * FQ), BF16),
        vm((NZ, 2, NT, M, 2 * FQ), BF16),
        vm((NZ, 2, NT, M, FQ), BF16),
        vm((NZ, *rows), BF16),
        vm(rows, BF16),
        vm((2, 2, 3 * NP, CAP, W), BF16),
        vm((2, 2, NP // 2, CAP, W), BF16),
        vm((T, RP), BF16),
        vm((2, T, 3 * RP + RP // 2), BF16),
        vm((2, NB, T, CB), BF16),
        vm((2, NB, T, CB), BF16),
        vm((NB, T, CB), F32),
        vm((2, NT, W, 2 * FQ), BF16),
        vm((2, FF, W), BF16),
        vm((NT, 8, T), F32),
        vm((NT, 8, T), F32),
        vm((T, W), BF16),
        vm((T, W), BF16),
        dma,
        dma((2,)),
        dma((2,)), dma((2,)),
        dma, dma((4,)),
        dma((4, 2)), dma((4, 2)),
        dma((2, 2, 2)),
        dma((5, 2)), dma((NZ, 2)),
        dma((NZ, 2)), dma((NZ, 2)),
        dma((NZ, 2)), dma((NZ, 2)),
        dma((NZ, 2)), dma((2,)),
        dma((2, 4, 2)),
        dma((2, 2, 2)),
        dma((3, 2)),
        dma((2, NB)), dma((2, NB)),
        dma,
    ]
    v = pl.BlockSpec(memory_space=pltpu.VMEM)
    a = pl.BlockSpec(memory_space=pl.ANY)
    return pl.pallas_call(
        functools.partial(layer_kernel, NP, NT),
        out_shape=jax.ShapeDtypeStruct((T, W), BF16),
        in_specs=[a, v, v, v, v, a, a, a],
        out_specs=a,
        scratch_shapes=scratch,
        compiler_params=pltpu.CompilerParams(
            collective_id=0, has_side_effects=True, vmem_limit_bytes=67043328
        ),
    )(
        tokens, routes.T, route_weights.T, norm_gain[None], final_gain[None],
        gate_weight, up_weight, down_weight,
    )


def solution(mesh):
    in_specs = (
        P("ep", "tp"),
        P("ep", None),
        P("ep", None),
        P("tp"),
        P("ep", "tp", None),
        P("ep", "tp", None),
        P("ep", None, "tp"),
        P("tp"),
    )
    out_specs = P("ep", "tp")
    return jax.shard_map(body, mesh=mesh, in_specs=in_specs, out_specs=out_specs, check_vma=False)
```

```python
import functools

import jax
import jax.numpy as jnp
from jax import lax
from jax.experimental import pallas as pl
from jax.experimental.pallas import tpu as pltpu
from jax.sharding import PartitionSpec as P

EPSILON = 1e-06
NZ = 8
F32 = jnp.float32
BF16 = jnp.bfloat16
I32 = jnp.int32


def layer_kernel(
    NP, NT, tok_hbm, rts, rws, ngain, fgain, gw, uw, dw, out,
    DB, MT, MR, XS, XR, PS, GS, GR, HB, OS, OR, RV, RW, CO, CM, RS, RD, ACC, WGU, WD, SQ, SQ2, OUT, SEL, SCA, PSQ, tok, tok_s,
    w_sem, sq_s, sq_r, mt_s, mt_r, db_s, db_r, ps_s, x_s, x_r, g_s, g_r, h_s, h_r,
    o_s, o_r, rv_r, rb_r, ob_s, rd_s, rd_r, out_s,
):
    T, W = tok.shape
    HALF = T // 2
    CAP = cap_of(T, NP)
    G2 = 2 * CAP
    RP = NP * G2
    M = NP * CAP
    FQ = WGU.shape[3] // 2
    CB = RS.shape[3]
    KA = 6 * NP * CAP
    NB = W // CB
    D = W * NT
    H = NP // 2
    NE = NZ * NP
    TB = min(128, T)
    ep = lax.axis_index("ep")
    y = lax.axis_index("tp")
    z = ep // NP
    p = ep % NP
    par = p % 2
    MESH = pl.DeviceIdType.MESH

    def zz(o):
        return (z + o + NZ) % NZ

    def at_plane(o, q):
        return {"ep": zz(o) * NP + q}

    def tdev(j):
        return {"tp": (y + j) % NT}

    def send(src, dst, ss, rs, dev):
        pltpu.make_async_remote_copy(
            src_ref=src, dst_ref=dst, send_sem=ss, recv_sem=rs, device_id=dev, device_id_type=MESH,
        ).start()

    def wait(ref, sem):
        pltpu.make_async_copy(ref, ref, sem).wait()

    barrier = pltpu.get_barrier_semaphore()

    def greet(j, carry):
        for o in (-3, -2, -1, 1, 2, 3):
            pl.semaphore_signal(barrier, inc=1, device_id=at_plane(o, j), device_id_type=MESH)
        return carry

    lax.fori_loop(0, NP, greet, 0)
    for j in range(1, NP):
        pl.semaphore_signal(barrier, inc=1, device_id=at_plane(0, (p + j) % NP), device_id_type=MESH)
    for j in range(1, NT):
        pl.semaphore_signal(barrier, inc=1, device_id=tdev(j), device_id_type=MESH)

    pltpu.make_async_copy(tok_hbm, tok, tok_s).start()
    wait(tok, tok_s)
    for m in range(2):
        for q in range(NT):
            cols = pl.ds(q * FQ, FQ)
            pltpu.make_async_copy(gw.at[m, :, cols], WGU.at[m, q, :, pl.ds(0, FQ)], w_sem.at[0]).start()
            pltpu.make_async_copy(uw.at[m, :, cols], WGU.at[m, q, :, pl.ds(FQ, FQ)], w_sem.at[0]).start()
    pltpu.make_async_copy(dw, WD, w_sem.at[1]).start()

    def squares(load, buf):
        for b in range(T // TB):
            v = load(b)
            s = jnp.sum(v * v, axis=1, keepdims=True)
            row = jnp.transpose(jnp.broadcast_to(s, (TB, 128)))
            buf[y, :, b * TB:(b + 1) * TB] = row[0:8, :]

    def share(buf, k):
        for j in range(1, NT):
            send(buf.at[y], buf.at[y], sq_s.at[k], sq_r.at[k], tdev(j))

    def scale_rows(buf):
        total = buf[0]
        for q in range(1, NT):
            total = total + buf[q]
        return lax.rsqrt(total / D + EPSILON)

    def send_h(h):
        part = tok.at[pl.ds(h * HALF, HALF)]
        send(part, DB.at[0, h], db_s.at[0, h], db_r.at[0, h], at_plane(1, p))
        send(part, DB.at[1, h], db_s.at[1, h], db_r.at[1, h], at_plane(-1, p))

    pl.semaphore_wait(barrier, 7 * NP - 1 + NT - 1)
    send_h(0)
    squares(lambda b: tok[b * TB:(b + 1) * TB, :].astype(F32), SQ)
    share(SQ, 0)

    r0 = rts[0:1, :]
    r1 = rts[1:2, :]
    eio = lax.broadcasted_iota(I32, (NE * 2, T), 0)
    oh0 = jnp.where(eio == r0, 1.0, 0.0)
    oh1 = jnp.where(eio == r1, 1.0, 0.0)
    up = jnp.where(
        lax.broadcasted_iota(I32, (T, T), 0) < lax.broadcasted_iota(I32, (T, T), 1), 1.0, 0.0
    ).astype(BF16)
    before = jnp.dot((oh0 + oh1).astype(BF16), up, preferred_element_type=F32)
    t0 = r0.astype(F32) * CAP + jnp.sum(oh0 * before, axis=0, keepdims=True)
    t1 = r1.astype(F32) * CAP + jnp.sum(oh1 * before, axis=0, keepdims=True)

    def near(k):
        wait(SQ.at[pl.ds(0, NT - 1)], sq_r.at[0])
        sub = lax.broadcasted_iota(I32, (8, T), 0)
        meta = jnp.where(sub == 0, t0, jnp.where(sub == 1, t1, scale_rows(SQ)))
        meta = jnp.where(sub == 2, rws[0:1, :], jnp.where(sub == 3, rws[1:2, :], meta))
        MT[...] = meta
        for slot, o in enumerate((1, -1, 2, -2)):
            send(MT, MR.at[slot], mt_s, mt_r.at[slot], at_plane(o, p))

    near(0)
    send_h(1)

    def choose(meta, at):
        hit = (at == meta[0:1, :]) | (at == meta[1:2, :])
        scale = jnp.sum(jnp.where(hit, meta[4:5, :], 0.0), axis=1, keepdims=True)
        return jnp.where(hit, 1.0, 0.0).astype(BF16), scale

    def pick(meta, at, xs, dst, chosen=None):
        sel, scale = chosen or choose(meta, at)
        rows = sel.shape[0]

        def cols(n, carry):
            cc = pl.ds(pl.multiple_of(n * CB, CB), CB)
            got = jnp.dot(sel[:, :HALF], xs[0][:, cc], preferred_element_type=F32)
            got = got + jnp.dot(sel[:, HALF:], xs[1][:, cc], preferred_element_type=F32)
            got = got * scale * ngain[0:1, cc]
            dst[:, :, :, cc] = got.astype(BF16).reshape(2, rows // G2, CAP, CB)
            return carry

        lax.fori_loop(0, NB, cols, 0)

    def row_index(rows, spread=1):
        r = lax.broadcasted_iota(I32, (rows, T), 0)
        half = rows // 2
        return (r % half) // CAP * (G2 * spread) + r // half * CAP + r % CAP

    def stage_a(i):
        at = (row_index(RP) + z * RP).astype(F32)
        if i == 0:
            pick(MT, at, (tok.at[pl.ds(0, HALF)], tok.at[pl.ds(HALF, HALF)]), XS.at[0])
        else:
            wait_meta(i - 1)
            for h in range(2):
                wait_dense(i - 1, h)
            pick(MR.at[i - 1], at, (DB.at[i - 1, 0], DB.at[i - 1, 1]), XS.at[i])
        for m in range(2):
            for j in range(1, NP):
                q = (p + j) % NP
                send(XS.at[i, m, q], XR.at[i, m, p], x_s.at[i, m], x_r.at[i, m], at_plane(0, q))
        for m in range(2):
            XR[i, m, p] = XS[i, m, p]

    arrived = set()

    def wait_dense(k, h):
        if (k, h) not in arrived:
            arrived.add((k, h))
            wait(DB.at[k, h], db_r.at[k, h])

    def wait_meta(k):
        if k not in arrived:
            arrived.add(k)
            wait(MR.at[k], mt_r.at[k])

    def forward(h):
        for k in range(2):
            wait_dense(k, h)
            send(DB.at[k, h], DB.at[2 + k, h], db_s.at[2 + k, h], db_r.at[2 + k, h], at_plane(1 - 2 * k, p))

    chosen = {}

    def far3(k):
        step = 1 - 2 * k
        if not chosen:
            for c in range(2):
                wait_meta(2 + c)
                SEL[c], SCA[c] = choose(MR.at[2 + c], (row_index(RP) + zz(1 - 2 * c) * RP).astype(F32))
                chosen[c] = True
        for h in range(2):
            wait_dense(2 + k, h)
        xs = (DB.at[2 + k, 0], DB.at[2 + k, 1])
        pick(MR.at[2 + k], None, xs, PS.at[k, :, pl.ds(0, NP)], (SEL[k], SCA[k]))
        for m in range(2):
            for j in range(NP):
                q = (p + j) % NP
                send(PS.at[k, m, q], XR.at[5 + k, m, p], ps_s.at[k, 0, m], x_r.at[5 + k, m], at_plane(step, q))

    def far4(k):
        step = 1 - 2 * k
        xs = (DB.at[2 + k, 0], DB.at[2 + k, 1])
        at = row_index(RP // 2, 2) + (zz(2 * step) * RP + k * G2)
        pick(MR.at[2 + k], at.astype(F32), xs, PS.at[k, :, pl.ds(NP, H)])
        for m in range(2):
            for j in range(H):
                q = (p // 2 + j) % H
                send(PS.at[k, m, NP + q], XR.at[7, m, p], ps_s.at[k, 1, m], x_r.at[7, m], at_plane(2 * step, 2 * q + k))

    def stage_b(i, m):
        wait(XR.at[i, m, pl.ds(0, NP - 1)] if i <= 4 else XR.at[i, m], x_r.at[i, m])

        def one(j, carry):
            q = (y + 1 + j) % NT
            rows = XR[i, m].reshape(M, W)
            got = jnp.dot(rows, WGU[m, q], preferred_element_type=F32)
            GS[i, m, q] = got.astype(BF16)

            @pl.when(j < NT - 1)
            def _():
                send(GS.at[i, m, q], GR.at[i, m, y], g_s.at[i, m], g_r.at[i, m], {"tp": q})

            return carry

        lax.fori_loop(0, NT, one, 0)

    def stage_c(i, m):
        wait(GR.at[i, m, pl.ds(0, NT - 1)], g_r.at[i, m])
        total = GS[i, m, y].astype(F32)
        for j in range(1, NT):
            total = total + GR[i, m, (y + j) % NT].astype(F32)
        gate = total[:, :FQ]
        HB[i, m, y] = (gate / (1.0 + jnp.exp(-gate)) * total[:, FQ:]).astype(BF16)
        for j in range(1, NT):
            send(HB.at[i, m, y], HB.at[i, m, y], h_s.at[i, m], h_r.at[i, m], tdev(j))

    def stage_d(i, m):
        wait(HB.at[i, m, pl.ds(0, NT - 1)], h_r.at[i, m])
        hid = jnp.concatenate([HB[i, m, q] for q in range(NT)], axis=1)

        def cols(n, carry):
            cc = pl.ds(pl.multiple_of(n * CB, CB), CB)
            got = jnp.dot(hid, WD[m, :, cc], preferred_element_type=F32)
            OS[i, m, :, :, cc] = got.astype(BF16).reshape(NP, CAP, CB)
            return carry

        lax.fori_loop(0, NB, cols, 0)
        if i == 0:
            for j in range(1, NP):
                q = (p + j) % NP
                send(OS.at[0, m, q], OR.at[m, p], o_s.at[0, m], o_r.at[m], at_plane(0, q))
            OR[m, p] = OS[0, m, p]
        else:
            returns(i, m, 0 if i in LATE else None)

    LATE = (3, 4, 7)

    def returns(i, m, part):
        cc = pl.ds(0, W) if part is None else pl.ds(part * (W // 2), W // 2)
        d = (i + 1) // 2
        ssem = o_s.at[i, m] if part != 1 else ob_s.at[LATE.index(i), m]
        for j in range(1 if d == 1 else 0, NP):
            q = (p + j) % NP
            if i < 7:
                side = (i + 1) % 2
                there = at_plane((d - 1) * (2 * side - 1), q)
                dst = RV.at[side, m, (d - 1) * NP + p, :, cc]
            else:
                side = 1 - par
                there = at_plane(3 - 6 * par, q)
                dst = RW.at[side, m, p // 2, :, cc]
            rsem = rv_r.at[side, d - 1, m] if part != 1 else rb_r.at[side, d // 4, m]
            send(OS.at[i, m, q, :, cc], dst, ssem, rsem, there)
        if d == 1:
            RV[side, m, p] = OS[i, m, p]

    def matrix(meta, at, b):
        bb = slice(b * TB, (b + 1) * TB)
        cols = [jnp.transpose(jnp.broadcast_to(meta[r:r + 1, bb], (128, TB))) for r in range(4)]
        out = []
        for a in at:
            out.append(jnp.where(a == cols[0], cols[2], 0.0) + jnp.where(a == cols[1], cols[3], 0.0))
        return jnp.concatenate(out, axis=1).astype(BF16)

    def lanes(base):
        return lax.broadcasted_iota(I32, (TB, 128), 1) + base

    def mats(k):
        def place(col, groups, step):
            m = col // (groups * CAP)
            r = col % (groups * CAP)
            return r // CAP % NP * (G2 * step) + m * CAP + r % CAP

        own = [(z * RP + place(lanes(c * 128), NP, 1)).astype(F32) for c in range(RP // 128)]
        for b in range(T // TB):
            CO[b * TB:(b + 1) * TB, :] = matrix(MT, own, b)
        for side in range(2):
            wait_meta(side)
            s = 1 - 2 * side
            at = []
            for c in range(KA // 128):
                col = lanes(c * 128)
                d = col % (KA // 2) // (NP * CAP)
                plane = jnp.where(d == 0, z, jnp.where(d == 1, zz(s), zz(2 * s)))
                at.append((plane * RP + place(col, 3 * NP, 1)).astype(F32))
            for c in range(RP // 256):
                col = place(lanes(c * 128), H, 2)
                at.append((col + (zz(3 * s) * RP + (1 - side) * G2)).astype(F32))
            for b in range(T // TB):
                CM[side, b * TB:(b + 1) * TB, :] = matrix(MR.at[side], at, b)

    def own_part(k):
        for m in range(2):
            wait(OR.at[m, pl.ds(0, NP - 1)], o_r.at[m])

        def cols(n, carry):
            cc = pl.ds(pl.multiple_of(n * CB, CB), CB)
            ACC[n] = jnp.dot(CO[...], OR[:, :, :, cc].reshape(RP, CB), preferred_element_type=F32)
            return carry

        lax.fori_loop(0, NB, cols, 0)

    def relay(k):
        cc = pl.ds(k * (W // 2), W // 2)
        for m in range(2):
            for side in range(2):
                if k == 0:
                    wait(RV.at[side, m, pl.ds(0, NP - 1)], rv_r.at[side, 0, m])
                    wait(RV.at[side, m, pl.ds(2 * NP, NP)], rv_r.at[side, 2, m])
                wait(RV.at[side, m, pl.ds(NP, NP), :, cc], (rb_r if k else rv_r).at[side, 1 - k, m])
                wait(RW.at[side, m, :, :, cc], rb_r.at[side, 1, m] if k else rv_r.at[side, 3, m])

        def cols(n, carry):
            cc = pl.ds(pl.multiple_of(n * CB, CB), CB)
            for side in range(2):
                rows = RV[side, :, :, :, cc].reshape(KA, CB)
                more = RW[side, :, :, :, cc].reshape(RP // 2, CB)
                got = jnp.dot(CM[side, :, :KA], rows, preferred_element_type=F32)
                got = got + jnp.dot(CM[side, :, KA:], more, preferred_element_type=F32)
                RS[side, n] = got.astype(BF16)
                send(RS.at[side, n], RD.at[side, n], rd_s.at[side, n], rd_r.at[side, n], at_plane(2 * side - 1, p))
            return carry

        lax.fori_loop(k * NB // 2, (k + 1) * NB // 2, cols, 0)

    stage_a(0)
    wait(WGU, w_sem.at[0])
    stage_b(0, 0)
    stage_c(0, 0)
    forward(0)
    stage_b(0, 1)
    wait(WD, w_sem.at[1])
    stage_d(0, 0)
    stage_a(2)
    stage_c(0, 1)
    forward(1)
    stage_a(1)
    stage_b(2, 0)
    stage_b(2, 1)
    stage_d(0, 1)
    stage_b(1, 1)
    mats(0)
    stage_c(2, 0)
    stage_c(2, 1)
    stage_b(1, 0)
    far3(0)
    far3(1)
    far4(0)
    stage_c(1, 0)
    far4(1)
    stage_c(1, 1)
    stage_b(5, 0)
    stage_b(6, 0)
    stage_a(4)
    stage_c(5, 0)
    stage_a(3)
    stage_c(6, 0)
    stage_b(5, 1)
    stage_d(5, 0)
    stage_b(6, 1)
    stage_b(7, 0)
    stage_d(6, 0)
    stage_c(5, 1)
    stage_c(6, 1)
    stage_b(4, 0)
    stage_b(7, 1)
    stage_b(4, 1)
    stage_d(5, 1)
    stage_d(6, 1)
    stage_c(7, 0)
    stage_b(3, 1)
    stage_d(2, 0)
    stage_d(1, 0)
    stage_d(7, 0)
    returns(7, 0, 1)
    stage_c(4, 1)
    stage_c(4, 0)
    stage_d(2, 1)
    stage_c(3, 1)
    stage_c(7, 1)
    stage_b(3, 0)
    stage_d(4, 0)
    own_part(0)
    stage_d(3, 1)
    stage_d(7, 1)
    stage_d(4, 1)
    returns(7, 1, 1)
    stage_d(1, 1)
    stage_c(3, 0)
    stage_d(3, 0)
    returns(3, 1, 1)
    returns(4, 0, 1)
    returns(4, 1, 1)
    returns(3, 0, 1)
    relay(0)
    relay(1)

    def finish(n, carry):
        for side in range(2):
            wait(RD.at[side, n], rd_r.at[side, n])
        total = ACC[n] + RD[0, n].astype(F32) + RD[1, n].astype(F32)
        ACC[n] = total
        part = total * total
        PSQ[n] = part[:, :128] + part[:, 128:] if CB == 256 else part
        return carry

    lax.fori_loop(0, NB, finish, 0)

    for b in range(T // TB):
        part = PSQ[0, b * TB:(b + 1) * TB, :]
        for n in range(1, NB):
            part = part + PSQ[n, b * TB:(b + 1) * TB, :]
        row = jnp.sum(part, axis=1, keepdims=True)
        SQ2[y, :, b * TB:(b + 1) * TB] = jnp.transpose(jnp.broadcast_to(row, (TB, 128)))[0:8, :]
    share(SQ2, 1)
    wait(SQ2.at[pl.ds(0, NT - 1)], sq_r.at[1])
    final = scale_rows(SQ2)
    for b in range(T // TB):
        sc = jnp.transpose(jnp.broadcast_to(final[0:1, b * TB:(b + 1) * TB], (128, TB)))
        for c in range(W // 128):
            n, l = c * 128 // CB, c * 128 % CB
            v = ACC[n, b * TB:(b + 1) * TB, l:l + 128] * sc * fgain[0:1, c * 128:(c + 1) * 128]
            OUT[b * TB:(b + 1) * TB, c * 128:(c + 1) * 128] = v.astype(BF16)
        pltpu.make_async_copy(OUT.at[pl.ds(b * TB, TB)], out.at[pl.ds(b * TB, TB)], out_s).start()

    for k in range(2):
        wait(SQ.at[pl.ds(0, NT - 1)], sq_s.at[k])
        for m in range(2):
            wait(PS.at[k, m, pl.ds(0, NP)], ps_s.at[k, 0, m])
            wait(PS.at[k, m, pl.ds(NP, H)], ps_s.at[k, 1, m])
        for n in range(NB):
            wait(RD.at[k, n], rd_s.at[k, n])
    wait(MR, mt_s)
    for k in range(4):
        for h in range(2):
            wait(DB.at[k, h], db_s.at[k, h])
    for i in range(NZ):
        for m in range(2):
            if i <= 4:
                wait(XR.at[i, m, pl.ds(0, NP - 1)], x_s.at[i, m])
            wait(GR.at[i, m, pl.ds(0, NT - 1)], g_s.at[i, m])
            wait(HB.at[i, m, pl.ds(0, NT - 1)], h_s.at[i, m])
            if i in LATE:
                for k, sem in enumerate((o_s.at[i, m], ob_s.at[LATE.index(i), m])):
                    wait(OS.at[i, m, :, :, pl.ds(k * (W // 2), W // 2)], sem)
            else:
                wait(OS.at[i, m, pl.ds(0, NP - 1)] if i <= 2 else OS.at[i, m], o_s.at[i, m])
    wait(OUT, out_s)


def cap_of(rows, planar):
    return 4 * rows // (NZ * planar * 2)


def body(tokens, routes, route_weights, norm_gain, gate_weight, up_weight, down_weight, final_gain):
    NT = lax.axis_size("tp")
    NP = lax.axis_size("ep") // NZ
    T, W = tokens.shape
    FF = gate_weight.shape[2]
    FQ = FF // NT
    CAP = cap_of(T, NP)
    G2 = 2 * CAP
    RP = NP * G2
    M = NP * CAP
    CB = 256 if W % 256 == 0 else 128
    NB = W // CB
    rows = (2, NP, CAP, W)
    vm = pltpu.VMEM
    dma = pltpu.SemaphoreType.DMA
    scratch = [
        vm((4, 2, T // 2, W), BF16),
        vm((8, T), F32),
        vm((4, 8, T), F32),
        vm((5, *rows), BF16),
        vm((NZ, *rows), BF16),
        vm((2, 2, NP + NP // 2, CAP, W), BF16),
        vm((NZ, 2, NT, M, 2 * FQ), BF16),
        vm((NZ, 2, NT, M, 2 * FQ), BF16),
        vm((NZ, 2, NT, M, FQ), BF16),
        vm((NZ, *rows), BF16),
        vm(rows, BF16),
        vm((2, 2, 3 * NP, CAP, W), BF16),
        vm((2, 2, NP // 2, CAP, W), BF16),
        vm((T, RP), BF16),
        vm((2, T, 3 * RP + RP // 2), BF16),
        vm((2, NB, T, CB), BF16),
        vm((2, NB, T, CB), BF16),
        vm((NB, T, CB), F32),
        vm((2, NT, W, 2 * FQ), BF16),
        vm((2, FF, W), BF16),
        vm((NT, 8, T), F32),
        vm((NT, 8, T), F32),
        vm((T, W), BF16),
        vm((2, RP, T), BF16),
        vm((2, RP, 1), F32),
        vm((NB, T, 128), F32),
        vm((T, W), BF16),
        dma,
        dma((2,)),
        dma((2,)), dma((2,)),
        dma, dma((4,)),
        dma((4, 2)), dma((4, 2)),
        dma((2, 2, 2)),
        dma((5, 2)), dma((NZ, 2)),
        dma((NZ, 2)), dma((NZ, 2)),
        dma((NZ, 2)), dma((NZ, 2)),
        dma((NZ, 2)), dma((2,)),
        dma((2, 4, 2)),
        dma((2, 2, 2)),
        dma((3, 2)),
        dma((2, NB)), dma((2, NB)),
        dma,
    ]
    v = pl.BlockSpec(memory_space=pltpu.VMEM)
    a = pl.BlockSpec(memory_space=pl.ANY)
    return pl.pallas_call(
        functools.partial(layer_kernel, NP, NT),
        out_shape=jax.ShapeDtypeStruct((T, W), BF16),
        in_specs=[a, v, v, v, v, a, a, a],
        out_specs=a,
        scratch_shapes=scratch,
        compiler_params=pltpu.CompilerParams(
            collective_id=0, has_side_effects=True, vmem_limit_bytes=67043328
        ),
    )(
        tokens, routes.T, route_weights.T, norm_gain[None], final_gain[None],
        gate_weight, up_weight, down_weight,
    )


def solution(mesh):
    in_specs = (
        P("ep", "tp"),
        P("ep", None),
        P("ep", None),
        P("tp"),
        P("ep", "tp", None),
        P("ep", "tp", None),
        P("ep", None, "tp"),
        P("tp"),
    )
    out_specs = P("ep", "tp")
    return jax.shard_map(body, mesh=mesh, in_specs=in_specs, out_specs=out_specs, check_vma=False)
```
